32 devices in a mesh: grp: 2 (over y), kv: 8 (over z, core), tp: 2 (over x).
Axes of the slice: x: 2, y: 2, z: 4, core: 2. Of those that a mesh axis runs over, the one named last changes fastest.
Arguments:
- tokens: bfloat16 [4096, 2048], P(('grp', 'kv')), parts along dimension 0, may hold values from -100 to 100
- query_weight: bfloat16 [2048, 512], P(None, 'tp'), may hold values from -0.125 to 0.125
- key_weight: bfloat16 [2048, 256], P(None, 'tp'), may hold values from -0.125 to 0.125
- value_weight: bfloat16 [2048, 256], P(None, 'tp'), may hold values from -0.125 to 0.125
- gate_weight: bfloat16 [2, 2048, 8], replicated, may hold values from -0.125 to 0.125
- squeeze_key: bfloat16 [2048, 64], replicated, may hold values from -0.125 to 0.125
- squeeze_value: bfloat16 [2048, 64], replicated, may hold values from -0.125 to 0.125
- out_weight: bfloat16 [512, 2048], P(None, 'tp'), may hold values from -1 to 1
- out_gain: bfloat16 [2048], replicated, may hold values from 0.099609375 to 1.8984375
- chosen: int32 [64, 32], P(('grp', 'kv')), parts along dimension 0, may hold values from -1 to 31, as said below
Outputs:
- output: bfloat16 [4096, 2048], P(('grp', 'kv'), 'tp'), parts along dimension 0
The draws below stay inside these ranges and needn't reach their ends.
There are 2 independent parts, one for each index of `grp`. The reference program is written for one: setup_inputs(seed, part) draws one part's arguments, and reference() takes and returns one part's arrays. A program takes and returns all parts, laid end to end along the dimension named above; an argument that names none is the same for every part. Nothing has to cross between parts.
Inputs may be any that keep to these rules, and one draw needn't show every extreme that they name: `chosen`: row n lists distinct key blocks no later than n, always n itself, the rest -1. The query blocks of one device together choose at most 2 distinct blocks of any other device, and some device reaches that.
All inputs are finite; a program needn't handle non-finite values.
Results may differ from the reference program's by a relative error of at most 0.01.
The reference program's roundings to bfloat16 on the way count: a program that leaves them out, or rounds other values in their place, can miss the bound.
Values may be sent and summed in bfloat16 or wider, within the bound.
A program may use at most 64 MiB of HBM per device.

```python
import jax
import jax.numpy as jnp
from jax import lax

D = 2048
HEADS = 8
KV_HEADS = 4
HEAD_DIM = 64
CMP_LEN = 32
SEL_BLOCK = 64
TOPN = 32
TOK_DEV = 256
TOKENS = 2048
NBLK = 32
N_KV = 8


def draw_tokens(key, part):
    key_one = jax.random.fold_in(key, 0)
    entries = jax.random.normal(key_one, (TOKENS, D), jnp.float32)
    entries = jnp.clip(entries, -6.0, 6.0)
    return entries.astype(jnp.bfloat16)


def draw_out_weight(key, part):
    row_count = HEADS * HEAD_DIM
    column = jnp.arange(D, dtype=jnp.float32) / float(max(D - 1, 1))
    entries = jnp.clip(jax.random.normal(key, (row_count, D), jnp.float32), -4.0, 4.0)
    growth = 3.0 ** column
    growth = growth / jnp.sqrt(jnp.mean(growth * growth))
    return (entries * growth[None, :] / jnp.sqrt(float(row_count))).astype(jnp.bfloat16)


def draw_chosen(key, part):
    per_device = TOK_DEV // SEL_BLOCK
    devices = N_KV
    key_pick, key_step, key_heat, key_noise = jax.random.split(key, 4)
    first_pick = jax.random.randint(key_pick, (devices, devices), 0, per_device)
    first_pick = first_pick.at[:, 0].set(0)
    second_pick = (first_pick + jax.random.randint(key_step, (devices, devices), 1, per_device)) % per_device
    block_ids = jnp.arange(NBLK, dtype=jnp.int32)
    query_device = block_ids // per_device
    block_owner = block_ids // per_device
    block_local = block_ids % per_device
    first_of = first_pick[query_device[:, None], block_owner[None, :]]
    second_of = second_pick[query_device[:, None], block_owner[None, :]]
    earlier = block_owner[None, :] < query_device[:, None]
    candidate = (block_local[None, :] == first_of) | (block_local[None, :] == second_of)
    same_device = (block_owner[None, :] == query_device[:, None]) & (block_ids[None, :] <= block_ids[:, None])
    member = earlier & candidate | same_device
    previous = (block_owner[None, :] == query_device[:, None] - 1) & candidate
    halfway = (block_owner[None, :] == query_device[:, None] - devices // 2) & (block_local[None, :] == first_of) & earlier
    forced = (block_ids[None, :] == block_ids[:, None]) | (block_ids[None, :] == 0) | previous | halfway
    heat = jax.random.randint(key_heat, (NBLK,), 0, 4)
    noise = jax.random.randint(key_noise, (NBLK, NBLK), 0, 4096)
    scores = (noise + heat[None, :] * 4096) * NBLK + block_ids[None, :]
    scores = scores + jnp.where(forced, 32768 * NBLK, 0)
    scores = jnp.where(member, scores, -1)
    top_scores, top_ids = lax.top_k(scores, TOPN)
    return jnp.where(top_scores >= 0, top_ids, -1).astype(jnp.int32)


def steps_of(own_key, extent, shards, least, top_value):
    loudness, own = 1.0, jax.random.fold_in(own_key, 6)
    for axis_at, blocks in shards:
        heights = jnp.exp(jax.random.uniform(jax.random.fold_in(own, axis_at), (blocks,), jnp.float32, least / len(shards), top_value / len(shards)))
        loudness = loudness * jnp.repeat(heights, extent[axis_at] // blocks).reshape([-1 if axis == axis_at else 1 for axis in range(len(extent))])
    return loudness


def gaussian(stream_key, shape, deviation, limit, cuts=(), kind=jnp.bfloat16):
    values = jax.random.normal(stream_key, shape, jnp.float32) * deviation
    if len(cuts) > 0:
        values = steps_of(stream_key, shape, cuts, -0.22, 0.18) * values
    return jnp.clip(values, min=-limit, max=limit).astype(kind)


def setup_inputs(seed: int = 0, part: int = 0) -> dict:
    key_of = jax.random.split(jax.random.key(seed), 11)
    own_keys = jax.random.split(jax.random.fold_in(key_of[10], part), 11)
    tokens = draw_tokens(jax.random.fold_in(jax.random.fold_in(key_of[10], part), 71), part)
    query_weight = gaussian(key_of[1], (D, HEADS * HEAD_DIM), D ** -0.5, 0.125, ((1, 2),))
    key_weight = gaussian(key_of[2], (D, KV_HEADS * HEAD_DIM), D ** -0.5, 0.125, ((1, 2),))
    value_weight = gaussian(key_of[3], (D, KV_HEADS * HEAD_DIM), D ** -0.5, 0.125, ((1, 2),))
    gate_weight = gaussian(key_of[4], (2, D, HEADS), D ** -0.5, 0.125)
    squeeze_key = gaussian(key_of[5], (CMP_LEN * HEAD_DIM, HEAD_DIM), (CMP_LEN * HEAD_DIM) ** -0.5, 0.125)
    squeeze_value = gaussian(key_of[6], (CMP_LEN * HEAD_DIM, HEAD_DIM), (CMP_LEN * HEAD_DIM) ** -0.5, 0.125)
    out_weight = draw_out_weight(jax.random.fold_in(key_of[10], 71), part)
    out_gain = jnp.clip(1.0 + 0.18 * jax.random.normal(key_of[8], (D,), jnp.float32), 0.099609375, 1.8984375).astype(jnp.bfloat16)
    chosen = draw_chosen(jax.random.fold_in(jax.random.fold_in(key_of[10], part), 71), part)
    return dict(tokens=tokens, query_weight=query_weight, key_weight=key_weight, value_weight=value_weight, gate_weight=gate_weight, squeeze_key=squeeze_key, squeeze_value=squeeze_value, out_weight=out_weight, out_gain=out_gain, chosen=chosen)


NEGATIVE = -1e+30
EPSILON = 1e-06

def masked_weights(scores, allowed):
    masked = jnp.where(allowed, scores, NEGATIVE)
    row_peak = lax.optimization_barrier(jnp.max(masked, axis=-1, keepdims=True))
    weights = jnp.where(allowed, jnp.exp(masked - row_peak), 0.0)
    weight_sum = lax.optimization_barrier(jnp.sum(weights, axis=-1, keepdims=True))
    return (weights.astype(jnp.bfloat16), weight_sum)

def reference(tokens, query_weight, key_weight, value_weight, gate_weight, squeeze_key, squeeze_value, out_weight, out_gain, chosen):
    head_size = HEAD_DIM
    group_size = HEADS // KV_HEADS
    score_scale = head_size ** (-0.5)
    queries = jnp.dot(tokens, query_weight, preferred_element_type=jnp.float32).astype(jnp.bfloat16)
    keys = jnp.dot(tokens, key_weight, preferred_element_type=jnp.float32).astype(jnp.bfloat16)
    values_all = jnp.dot(tokens, value_weight, preferred_element_type=jnp.float32).astype(jnp.bfloat16)
    gate_values = jax.nn.sigmoid(jnp.einsum('td,bdh->tbh', tokens.astype(jnp.float32), gate_weight.astype(jnp.float32)))
    squeeze_rows = TOKENS // CMP_LEN
    key_flat = keys.reshape(squeeze_rows, CMP_LEN, KV_HEADS, head_size).transpose(0, 2, 1, 3).reshape(squeeze_rows * KV_HEADS, CMP_LEN * head_size)
    value_flat = values_all.reshape(squeeze_rows, CMP_LEN, KV_HEADS, head_size).transpose(0, 2, 1, 3).reshape(squeeze_rows * KV_HEADS, CMP_LEN * head_size)
    summary_keys = jnp.dot(key_flat, squeeze_key, preferred_element_type=jnp.float32).astype(jnp.bfloat16).reshape(squeeze_rows, KV_HEADS, head_size)
    summary_values = jnp.dot(value_flat, squeeze_value, preferred_element_type=jnp.float32).astype(jnp.bfloat16).reshape(squeeze_rows, KV_HEADS, head_size)
    summary_end = jnp.arange(squeeze_rows, dtype=jnp.int32) * CMP_LEN + (CMP_LEN - 1)
    key_blocks = keys.reshape(NBLK, SEL_BLOCK, KV_HEADS, head_size)
    value_blocks = values_all.reshape(NBLK, SEL_BLOCK, KV_HEADS, head_size)
    query_blocks = queries.reshape(NBLK, SEL_BLOCK, KV_HEADS, group_size, head_size)

    def one_block(operands):
        block_queries, block_chosen, block_index = operands
        positions = block_index * SEL_BLOCK + jnp.arange(SEL_BLOCK, dtype=jnp.int32)
        wide_queries = block_queries.astype(jnp.float32)
        scores = jnp.einsum('qkgd,ckd->qkgc', wide_queries, summary_keys.astype(jnp.float32)) * score_scale
        allowed = (summary_end[None, :] <= positions[:, None])[:, None, None, :]
        weights, weight_sum = masked_weights(scores, allowed)
        squeezed = jnp.einsum('qkgc,ckd->qkgd', weights.astype(jnp.float32), summary_values.astype(jnp.float32)) / jnp.maximum(weight_sum, 1.0)
        safe_ids = jnp.maximum(block_chosen, 0).astype(jnp.int32)
        picked_keys = jnp.take(key_blocks, safe_ids, axis=0).reshape(TOPN * SEL_BLOCK, KV_HEADS, head_size)
        picked_values = jnp.take(value_blocks, safe_ids, axis=0).reshape(TOPN * SEL_BLOCK, KV_HEADS, head_size)
        key_positions = (safe_ids[:, None] * SEL_BLOCK + jnp.arange(SEL_BLOCK, dtype=jnp.int32)[None, :]).reshape(-1)
        usable = jnp.repeat(block_chosen >= 0, SEL_BLOCK)
        allowed = (usable[None, :] & (key_positions[None, :] <= positions[:, None]))[:, None, None, :]
        scores = jnp.einsum('qkgd,pkd->qkgp', wide_queries, picked_keys.astype(jnp.float32)) * score_scale
        weights, weight_sum = masked_weights(scores, allowed)
        selected = jnp.einsum('qkgp,pkd->qkgd', weights.astype(jnp.float32), picked_values.astype(jnp.float32)) / weight_sum
        return (squeezed, selected)
    squeezed, selected = lax.map(one_block, (query_blocks, chosen, jnp.arange(NBLK, dtype=jnp.int32)))
    squeezed = squeezed.reshape(TOKENS, HEADS, head_size)
    selected = selected.reshape(TOKENS, HEADS, head_size)
    mixed_heads = (gate_values[:, 0, :, None] * squeezed + gate_values[:, 1, :, None] * selected).reshape(TOKENS, HEADS * head_size).astype(jnp.bfloat16)
    projected = jnp.dot(mixed_heads, out_weight, preferred_element_type=jnp.float32)
    squares = lax.optimization_barrier(jnp.sum(projected * projected, axis=1, keepdims=True))
    return (projected * lax.rsqrt(squares / D + EPSILON) * out_gain.astype(jnp.float32)[None, :]).astype(jnp.bfloat16)
```

```python
import functools

import jax
import jax.numpy as jnp
from jax import lax
from jax.experimental import pallas as pl
from jax.experimental.pallas import tpu as pltpu
from jax.sharding import PartitionSpec as P

CMP_LEN = 32
SEL_BLOCK = 64
NEGATIVE = -1e30
EPSILON = 1e-06
MESH = pl.DeviceIdType.MESH
NT = (((1,), (1,)), ((), ()))


def kernel(
    n,
    dims,
    chosen_ref,
    tok_hbm,
    qw_hbm,
    kw_hbm,
    vw_hbm,
    gw_hbm,
    sqk_hbm,
    sqv_hbm,
    ow_hbm,
    out_ref,
    tok,
    weights,
    kw,
    vw,
    gw,
    sqk,
    sqv,
    ow,
    kv,
    kvf,
    summ,
    bias,
    q,
    gates,
    m_ref,
    l_ref,
    acc_ref,
    mix,
    sq,
    load_sem,
    recv_sem,
    up_sem,
    across_sem,
    tp_send,
    tp_recv,
):
    rows, width, hs, kvl, group, total_cols, tps = dims
    chips = n // 2
    nq = rows // SEL_BLOCK
    qcols = kvl * group * hs
    feat = 2 * hs
    cmp_rows = rows // CMP_LEN
    unit = group * SEL_BLOCK
    me = lax.axis_index("kv")
    tp = lax.axis_index("tp")
    z = me // 2
    core = me - 2 * z
    mate = 2 * z + 1 - core
    has_up = z < chips - 1
    parts = kvl + 1

    kcols = kvl * hs
    joint = kcols % 128 == 0
    if joint:
        kw = weights.at[:, pl.ds(qcols, kcols)]
        vw = weights.at[:, pl.ds(qcols + kcols, kcols)]
    loads = [
        pltpu.make_async_copy(tok_hbm, tok, load_sem.at[0]),
        pltpu.make_async_copy(kw_hbm, kw, load_sem.at[1]),
        pltpu.make_async_copy(vw_hbm, vw, load_sem.at[2]),
        pltpu.make_async_copy(sqk_hbm, sqk, load_sem.at[3]),
        pltpu.make_async_copy(sqv_hbm, sqv, load_sem.at[4]),
        pltpu.make_async_copy(qw_hbm, weights.at[:, pl.ds(0, qcols)], load_sem.at[5]),
        pltpu.make_async_copy(gw_hbm, gw, load_sem.at[6]),
        pltpu.make_async_copy(ow_hbm, ow, load_sem.at[7]),
    ]
    for load in loads:
        load.start()

    barrier = pltpu.get_barrier_semaphore()
    pl.semaphore_signal(barrier, inc=1, device_id={"kv": mate}, device_id_type=MESH)
    for d in range(1, tps):
        pl.semaphore_signal(
            barrier, inc=1, device_id={"tp": lax.rem(tp + d, tps)}, device_id_type=MESH
        )

    @pl.when(z > 0)
    def _():
        pl.semaphore_signal(barrier, inc=1, device_id={"kv": me - 2}, device_id_type=MESH)

    ids = chosen_ref[...]
    lane_row = lax.broadcasted_iota(jnp.int32, (nq, rows), 1)

    def make_bias(j, carry):
        row = jnp.zeros((nq, rows), jnp.float32)
        for b in range(nq):
            hit = jnp.max(jnp.where(ids == j * nq + b, 1.0, 0.0), axis=1, keepdims=True)
            here = (lane_row >= b * SEL_BLOCK) & (lane_row < (b + 1) * SEL_BLOCK)
            row = jnp.where(here, hit, row)
        bias[j, 0:nq, :] = jnp.where(row > 0.5, 0.0, NEGATIVE)
        return carry

    lax.fori_loop(0, me + 1, make_bias, 0)

    def clear(j, carry):
        summ[j] = jnp.zeros((cmp_rows, kvl * feat), jnp.float32)
        return carry

    lax.fori_loop(me + 1, n, clear, 0)

    for i in range(3):
        loads[i].wait()
    if joint:
        pairs = jnp.dot(
            tok[...], weights[:, qcols : qcols + 2 * kcols], preferred_element_type=jnp.float32
        )
        sides = [pairs[:, :kcols], pairs[:, kcols:]]
    else:
        sides = [
            jnp.dot(tok[...], w[...], preferred_element_type=jnp.float32) for w in (kw, vw)
        ]
    sides = [side.astype(jnp.bfloat16).astype(jnp.float32) for side in sides]
    for i, side in enumerate(sides):
        if not joint:
            side = jnp.concatenate([side, jnp.zeros((rows, 128 - kcols), jnp.float32)], axis=1)
        kvf[i] = side
    for k in range(kvl):
        kv[me, k] = jnp.concatenate(
            [side[:, k * hs : (k + 1) * hs] for side in sides], axis=1
        ).astype(jnp.bfloat16)

    def piece(source, part):
        return summ.at[source] if part == kvl else kv.at[source, part]

    def upward(source, part):
        return pltpu.make_async_remote_copy(
            src_ref=piece(source, part),
            dst_ref=piece(source, part),
            send_sem=up_sem.at[source // 2, part],
            recv_sem=recv_sem.at[source, part],
            device_id={"kv": me + 2},
            device_id_type=MESH,
        )

    def across(source, part):
        return pltpu.make_async_remote_copy(
            src_ref=piece(source, part),
            dst_ref=piece(source, part),
            send_sem=across_sem.at[source // 2, part],
            recv_sem=recv_sem.at[source, part],
            device_id={"kv": mate},
            device_id_type=MESH,
        )

    pl.semaphore_wait(barrier, tps + jnp.minimum(chips - 1 - z, 1))

    def send_own(part):
        @pl.when(has_up)
        def _():
            upward(me, part).start()

        @pl.when(core == 0)
        def _():
            across(me, part).start()

    for k in range(kvl):
        send_own(k)

    loads[3].wait()
    loads[4].wait()
    squeezed = []
    for side, weight in ((0, sqk), (1, sqv)):
        tiles = []
        for p in range(0, CMP_LEN, 2):
            a = kvf[side, pl.ds(p, cmp_rows, stride=CMP_LEN), :]
            b = kvf[side, pl.ds(p + 1, cmp_rows, stride=CMP_LEN), :]
            heads = [
                jnp.concatenate([x[:, k * hs : (k + 1) * hs] for x in (a, b)], axis=1)
                for k in range(kvl)
            ]
            tiles.append(jnp.concatenate(heads, axis=0))
        flat = jnp.concatenate(tiles, axis=1).astype(jnp.bfloat16)
        squeezed.append(
            lax.dot_general(flat, weight[...], NT, preferred_element_type=jnp.float32)
            .astype(jnp.bfloat16)
            .astype(jnp.float32)
        )
    summ[me] = jnp.concatenate(
        [
            half[k * cmp_rows : (k + 1) * cmp_rows]
            for k in range(kvl)
            for half in squeezed
        ],
        axis=1,
    )
    send_own(kvl)

    loads[5].wait()
    scale = hs ** (-0.5)
    queries = (
        jnp.dot(tok[...], weights[:, :qcols], preferred_element_type=jnp.float32)
        .astype(jnp.bfloat16)
        .astype(jnp.float32)
        * scale
    )
    low_q = lax.broadcasted_iota(jnp.int32, (SEL_BLOCK, feat), 1) < hs
    for k in range(kvl):
        for b in range(nq):
            tile = queries[b * SEL_BLOCK : (b + 1) * SEL_BLOCK, k * feat : (k + 1) * feat]
            q[k, b * unit : b * unit + SEL_BLOCK, :] = jnp.where(low_q, tile, 0.0).astype(
                jnp.bfloat16
            )
            q[k, b * unit + SEL_BLOCK : (b + 1) * unit, :] = jnp.where(
                low_q, pltpu.roll(tile, hs, 1), 0.0
            ).astype(jnp.bfloat16)
    loads[6].wait()
    hl = kvl * group
    every = jax.nn.sigmoid(
        lax.dot_general(tok[...], gw[...], NT, preferred_element_type=jnp.float32)
    )
    for branch in range(2):
        base = branch * tps * hl
        mine = every[:, base : base + hl]
        for t in range(1, tps):
            mine = jnp.where(tp == t, every[:, base + t * hl : base + (t + 1) * hl], mine)
        gates[branch] = mine

    def attend(source, k, first):
        keys = kv[source, k]
        for b in range(nq):
            at = pl.ds(b * unit, unit)
            s = lax.dot_general(q[k, at, :], keys, NT, preferred_element_type=jnp.float32)
            s = s + bias[source, b : b + 1, :]
            if first:
                col = lax.broadcasted_iota(jnp.int32, (SEL_BLOCK, rows), 1)
                row = lax.broadcasted_iota(jnp.int32, (SEL_BLOCK, rows), 0)
                seen = col <= row + b * SEL_BLOCK
                s = jnp.concatenate(
                    [
                        jnp.where(seen, s[:SEL_BLOCK], NEGATIVE),
                        jnp.where(seen, s[SEL_BLOCK:], NEGATIVE),
                    ],
                    axis=0,
                )
            peak = jnp.broadcast_to(jnp.max(s, axis=1, keepdims=True), (unit, feat))
            if not first:
                before = m_ref[k, at, :]
                peak = jnp.maximum(before, peak)
                alpha = jnp.exp(before - peak)
            p = jnp.exp(s - jnp.concatenate([peak] * (rows // feat), axis=1))
            sums = p[:, :feat]
            for i in range(1, rows // feat):
                sums = sums + p[:, i * feat : (i + 1) * feat]
            got = jnp.dot(p.astype(jnp.bfloat16), keys, preferred_element_type=jnp.float32)
            if not first:
                sums = sums + l_ref[k, at, :] * alpha
                got = got + acc_ref[k, at, :] * alpha
            m_ref[k, at, :] = peak
            l_ref[k, at, :] = sums
            acc_ref[k, at, :] = got

    for k in range(kvl):
        attend(me, k, True)

    @pl.when(core == 1)
    def _():
        for k in range(kvl):
            across(me - 1, k).wait_recv()
            attend(me - 1, k, False)
        across(me - 1, kvl).wait_recv()

    def step(s, carry):
        mine = me - 2 * s
        other = mate - 2 * s

        def take(part):
            upward(mine, part).wait_recv()

            @pl.when(has_up)
            def _():
                upward(mine, part).start()

            across(mine, part).start()

        for k in range(kvl):
            take(k)
            attend(mine, k, False)
            across(other, k).wait_recv()
            attend(other, k, False)
        take(kvl)
        across(other, kvl).wait_recv()
        return carry

    lax.fori_loop(1, z + 1, step, 0)

    cols = n * cmp_rows
    for k in range(kvl):
        small = (
            summ[:, :, k * feat : (k + 1) * feat].reshape(cols, feat).astype(jnp.bfloat16)
        )
        for b in range(nq):
            at = pl.ds(b * unit, unit)
            s = lax.dot_general(q[k, at, :], small, NT, preferred_element_type=jnp.float32)
            col = lax.broadcasted_iota(jnp.int32, (SEL_BLOCK, cols), 1)
            row = lax.broadcasted_iota(jnp.int32, (SEL_BLOCK, cols), 0)
            seen = col * CMP_LEN + (CMP_LEN - 1) <= row + (me * rows + b * SEL_BLOCK)
            s0 = jnp.where(seen, s[:SEL_BLOCK], NEGATIVE)
            s1 = jnp.where(seen, s[SEL_BLOCK:], NEGATIVE)
            halves = []
            for half in (s0, s1):
                peak = jnp.max(half, axis=1, keepdims=True)
                halves.append(jnp.where(seen, jnp.exp(half - peak), 0.0))
            w = jnp.concatenate(halves, axis=0)
            low_sum = jnp.sum(w, axis=1, keepdims=True)
            comp = jnp.dot(w.astype(jnp.bfloat16), small, preferred_element_type=jnp.float32)
            comp = comp / jnp.maximum(low_sum, 1.0)
            sel = acc_ref[k, at, :] / jnp.sum(l_ref[k, at, :], axis=1, keepdims=True)
            pos = pl.ds(b * SEL_BLOCK, SEL_BLOCK)
            heads = []
            for g in range(group):
                h = k * group + g
                cut = slice(g * SEL_BLOCK, (g + 1) * SEL_BLOCK)
                heads.append(
                    gates[0, pos, h : h + 1] * comp[cut] + gates[1, pos, h : h + 1] * sel[cut]
                )
            mix[tp, pos, k * feat : (k + 1) * feat] = jnp.where(
                low_q, pltpu.roll(heads[0], hs, 1), heads[1]
            ).astype(jnp.bfloat16)

    def swap(ref, d, source, kind):
        return pltpu.make_async_remote_copy(
            src_ref=ref.at[source],
            dst_ref=ref.at[source],
            send_sem=tp_send.at[kind, d],
            recv_sem=tp_recv.at[kind, source],
            device_id={"tp": lax.rem(tp + d, tps)},
            device_id_type=MESH,
        )

    for d in range(1, tps):
        swap(mix, d, tp, 0).start()
    loads[7].wait()
    for d in range(1, tps):
        swap(mix, d, lax.rem(tp + d, tps), 0).wait_recv()
    proj = jnp.dot(mix[0], ow[:qcols, :], preferred_element_type=jnp.float32)
    for t in range(1, tps):
        proj = proj + jnp.dot(
            mix[t], ow[t * qcols : (t + 1) * qcols, :], preferred_element_type=jnp.float32
        )
    out_ref[...] = proj
    lanes = proj[:, :128] * proj[:, :128]
    for i in range(1, proj.shape[1] // 128):
        tile = proj[:, i * 128 : (i + 1) * 128]
        lanes = lanes + tile * tile
    sq[tp] = jnp.sum(lanes.T.reshape(16, 8, rows), axis=0)
    for d in range(1, tps):
        swap(sq, d, tp, 1).start()

    for part in range(parts):
        @pl.when(has_up)
        def _():
            upward(me, part).wait_send()

        @pl.when(core == 0)
        def _():
            across(me, part).wait_send()

    def drain(s, carry):
        mine = me - 2 * s
        for part in range(parts):
            @pl.when(has_up)
            def _():
                upward(mine, part).wait_send()

            across(mine, part).wait_send()
        return carry

    lax.fori_loop(1, z + 1, drain, 0)
    for d in range(1, tps):
        swap(sq, d, lax.rem(tp + d, tps), 1).wait_recv()
    squares = jnp.sum(jnp.sum(sq[...], axis=0), axis=0, keepdims=True)
    factor = lax.rsqrt(squares / total_cols + EPSILON)
    column = jnp.broadcast_to(factor, (128, rows)).T
    for i in range(out_ref.shape[1] // 128):
        out_ref[:, i * 128 : (i + 1) * 128] = out_ref[:, i * 128 : (i + 1) * 128] * column
    for d in range(1, tps):
        swap(mix, d, tp, 0).wait_send()
        swap(sq, d, tp, 1).wait_send()


def body(
    n,
    tps,
    tokens,
    query_weight,
    key_weight,
    value_weight,
    gate_weight,
    squeeze_key,
    squeeze_value,
    out_weight,
    out_gain,
    chosen,
):
    rows, width = tokens.shape
    hs = squeeze_key.shape[1]
    kvl = key_weight.shape[1] // hs
    qcols = query_weight.shape[1]
    group = qcols // hs // kvl
    cols = out_weight.shape[1]
    total_cols = out_gain.shape[0]
    feat = 2 * hs
    nq = rows // SEL_BLOCK
    stack = nq * group * SEL_BLOCK
    cmp_rows = rows // CMP_LEN
    dims = (rows, width, hs, kvl, group, total_cols, tps)
    kcols = kvl * hs
    joint = kcols % 128 == 0
    spare = (8, 128) if joint else (width, kcols)
    any_spec = pl.BlockSpec(memory_space=pl.ANY)
    vmem = pl.BlockSpec(memory_space=pltpu.VMEM)
    bf, f32 = jnp.bfloat16, jnp.float32
    dma = pltpu.SemaphoreType.DMA
    scaled = pl.pallas_call(
        functools.partial(kernel, n, dims),
        out_shape=jax.ShapeDtypeStruct((rows, cols), f32),
        in_specs=[vmem] + [any_spec] * 8,
        out_specs=vmem,
        scratch_shapes=[
            pltpu.VMEM((rows, width), bf),
            pltpu.VMEM((width, qcols + 2 * kcols if joint else qcols), bf),
            pltpu.VMEM(spare, bf),
            pltpu.VMEM(spare, bf),
            pltpu.VMEM((gate_weight.shape[0] * gate_weight.shape[2], width), bf),
            pltpu.VMEM(squeeze_key.shape[::-1], bf),
            pltpu.VMEM(squeeze_value.shape[::-1], bf),
            pltpu.VMEM(out_weight.shape, bf),
            pltpu.VMEM((n, kvl, rows, feat), bf),
            pltpu.VMEM((2, rows, max(kcols, 128)), f32),
            pltpu.VMEM((n, cmp_rows, kvl * feat), f32),
            pltpu.VMEM((n, 8, rows), f32),
            pltpu.VMEM((kvl, stack, feat), bf),
            pltpu.VMEM((2, rows, kvl * group), f32),
            pltpu.VMEM((kvl, stack, feat), f32),
            pltpu.VMEM((kvl, stack, feat), f32),
            pltpu.VMEM((kvl, stack, feat), f32),
            pltpu.VMEM((tps, rows, qcols), bf),
            pltpu.VMEM((tps, 8, rows), f32),
            dma((8,)),
            dma((n, kvl + 1)),
            dma((n // 2, kvl + 1)),
            dma((n // 2, kvl + 1)),
            dma((2, tps)),
            dma((2, tps)),
        ],
        compiler_params=pltpu.CompilerParams(
            collective_id=0, has_side_effects=True, vmem_limit_bytes=56 * 1024 * 1024
        ),
    )(
        chosen,
        tokens,
        query_weight,
        key_weight,
        value_weight,
        gate_weight.transpose(0, 2, 1).reshape(-1, width),
        squeeze_key.T,
        squeeze_value.T,
        out_weight,
    )
    gain = lax.dynamic_slice_in_dim(out_gain, lax.axis_index("tp") * cols, cols, 0)
    return (scaled * gain.astype(f32)[None, :]).astype(bf)


def solution(mesh):
    in_specs = (
        P(("grp", "kv"), None),
        P(None, "tp"),
        P(None, "tp"),
        P(None, "tp"),
        P(),
        P(),
        P(),
        P(None, "tp"),
        P(),
        P(("grp", "kv"), None),
    )
    return jax.shard_map(
        functools.partial(body, mesh.shape["kv"], mesh.shape["tp"]),
        mesh=mesh,
        in_specs=in_specs,
        out_specs=P(("grp", "kv"), "tp"),
        check_vma=False,
    )
```

```python
import functools

import jax
import jax.numpy as jnp
from jax import lax
from jax.experimental import pallas as pl
from jax.experimental.pallas import tpu as pltpu
from jax.sharding import PartitionSpec as P

CMP_LEN = 32
SEL_BLOCK = 64
NEGATIVE = -1e30
EPSILON = 1e-06
MESH = pl.DeviceIdType.MESH
NT = (((1,), (1,)), ((), ()))


def kernel(
    n,
    dims,
    chosen_ref,
    gain_ref,
    tok_hbm,
    qw_hbm,
    kw_hbm,
    vw_hbm,
    gw_hbm,
    sqk_hbm,
    sqv_hbm,
    ow_hbm,
    out_ref,
    tok,
    weights,
    kw,
    vw,
    gw,
    sqk,
    sqv,
    ow,
    keys,
    vals,
    kvf,
    summ,
    bias,
    q,
    gates,
    m_ref,
    l_ref,
    acc_ref,
    s_ref,
    p_ref,
    mix,
    sq,
    load_sem,
    recv_sem,
    up_sem,
    across_sem,
    tp_send,
    tp_recv,
):
    rows, width, hs, kvl, group, total_cols, tps = dims
    chips = n // 2
    nq = rows // SEL_BLOCK
    qcols = kvl * group * hs
    cmp_rows = rows // CMP_LEN
    lanes_q = group * rows
    me = lax.axis_index("kv")
    tp = lax.axis_index("tp")
    z = me // 2
    core = me - 2 * z
    mate = 2 * z + 1 - core
    has_up = z < chips - 1
    parts = 3

    kcols = kvl * hs
    joint = kcols % 128 == 0
    if joint:
        kw = weights.at[:, pl.ds(qcols, kcols)]
        vw = weights.at[:, pl.ds(qcols + kcols, kcols)]
    loads = [
        pltpu.make_async_copy(tok_hbm, tok, load_sem.at[0]),
        pltpu.make_async_copy(kw_hbm, kw, load_sem.at[1]),
        pltpu.make_async_copy(vw_hbm, vw, load_sem.at[2]),
        pltpu.make_async_copy(sqk_hbm, sqk, load_sem.at[3]),
        pltpu.make_async_copy(sqv_hbm, sqv, load_sem.at[4]),
        pltpu.make_async_copy(qw_hbm, weights.at[:, pl.ds(0, qcols)], load_sem.at[5]),
        pltpu.make_async_copy(gw_hbm, gw, load_sem.at[6]),
        pltpu.make_async_copy(ow_hbm, ow, load_sem.at[7]),
    ]
    for load in loads:
        load.start()

    barrier = pltpu.get_barrier_semaphore()
    pl.semaphore_signal(barrier, inc=1, device_id={"kv": mate}, device_id_type=MESH)
    for d in range(1, tps):
        pl.semaphore_signal(
            barrier, inc=1, device_id={"tp": lax.rem(tp + d, tps)}, device_id_type=MESH
        )

    @pl.when(z > 0)
    def _():
        pl.semaphore_signal(barrier, inc=1, device_id={"kv": me - 2}, device_id_type=MESH)

    ids = chosen_ref[...]

    def make_bias(j, carry):
        for b in range(nq):
            hit = jnp.max(jnp.where(ids == j * nq + b, 0.0, NEGATIVE), axis=1, keepdims=True)
            hit = jnp.broadcast_to(hit, (nq, SEL_BLOCK))
            bias[j, b : b + 1, :] = jnp.concatenate(
                [hit[i : i + 1, :] for i in range(nq)] * group, axis=1
            )
        return carry

    lax.fori_loop(0, me + 1, make_bias, 0)

    def clear(j, carry):
        summ[j] = jnp.zeros((cmp_rows, 2 * kcols), jnp.float32)
        return carry

    lax.fori_loop(me + 1, n, clear, 0)

    for i in range(3):
        loads[i].wait()
    if joint:
        pairs = jnp.dot(
            tok[...], weights[:, qcols : qcols + 2 * kcols], preferred_element_type=jnp.float32
        )
        sides = [pairs[:, :kcols], pairs[:, kcols:]]
    else:
        sides = [
            jnp.dot(tok[...], w[...], preferred_element_type=jnp.float32) for w in (kw, vw)
        ]
    sides = [side.astype(jnp.bfloat16).astype(jnp.float32) for side in sides]
    for i, side in enumerate(sides):
        if not joint:
            side = jnp.concatenate([side, jnp.zeros((rows, 128 - kcols), jnp.float32)], axis=1)
        kvf[i] = side
    keys[me] = sides[0].astype(jnp.bfloat16)
    vals[me] = sides[1].T.astype(jnp.bfloat16)

    def piece(source, part):
        return (keys, vals, summ)[part].at[source]

    def upward(source, part):
        return pltpu.make_async_remote_copy(
            src_ref=piece(source, part),
            dst_ref=piece(source, part),
            send_sem=up_sem.at[source // 2, part],
            recv_sem=recv_sem.at[source, part],
            device_id={"kv": me + 2},
            device_id_type=MESH,
        )

    def across(source, part):
        return pltpu.make_async_remote_copy(
            src_ref=piece(source, part),
            dst_ref=piece(source, part),
            send_sem=across_sem.at[source // 2, part],
            recv_sem=recv_sem.at[source, part],
            device_id={"kv": mate},
            device_id_type=MESH,
        )

    pl.semaphore_wait(barrier, tps + jnp.minimum(chips - 1 - z, 1))

    def send_own(part):
        @pl.when(has_up)
        def _():
            upward(me, part).start()

        @pl.when(core == 0)
        def _():
            across(me, part).start()

    send_own(0)
    send_own(1)

    loads[3].wait()
    loads[4].wait()
    squeezed = []
    for side, weight in ((0, sqk), (1, sqv)):
        tiles = []
        for p in range(0, CMP_LEN, 2):
            a = kvf[side, pl.ds(p, cmp_rows, stride=CMP_LEN), :]
            b = kvf[side, pl.ds(p + 1, cmp_rows, stride=CMP_LEN), :]
            heads = [
                jnp.concatenate([x[:, k * hs : (k + 1) * hs] for x in (a, b)], axis=1)
                for k in range(kvl)
            ]
            tiles.append(jnp.concatenate(heads, axis=0))
        flat = jnp.concatenate(tiles, axis=1).astype(jnp.bfloat16)
        squeezed.append(
            lax.dot_general(flat, weight[...], NT, preferred_element_type=jnp.float32)
            .astype(jnp.bfloat16)
            .astype(jnp.float32)
        )
    summ[me] = jnp.concatenate(
        [
            half[k * cmp_rows : (k + 1) * cmp_rows]
            for half in squeezed
            for k in range(kvl)
        ],
        axis=1,
    )
    send_own(2)

    loads[5].wait()
    scale = hs ** (-0.5)
    queries = (
        jnp.dot(tok[...], weights[:, :qcols], preferred_element_type=jnp.float32)
        .astype(jnp.bfloat16)
        .astype(jnp.float32)
        * scale
    )
    turned = queries.T.astype(jnp.bfloat16)
    for k in range(kvl):
        q[k] = jnp.zeros((kcols, lanes_q), jnp.bfloat16)
        for g in range(group):
            h = k * group + g
            q[k, k * hs : (k + 1) * hs, g * rows : (g + 1) * rows] = turned[
                h * hs : (h + 1) * hs, :
            ]
    loads[6].wait()
    hl = kvl * group
    every = jax.nn.sigmoid(
        lax.dot_general(gw[...], tok[...], NT, preferred_element_type=jnp.float32)
    )
    for branch in range(2):
        base = branch * tps * hl
        mine = every[base : base + hl, :]
        for t in range(1, tps):
            mine = jnp.where(tp == t, every[base + t * hl : base + (t + 1) * hl, :], mine)
        gates[branch, 0:hl, :] = mine

    def weigh(source, first):
        for k in range(kvl):
            s_ref[k] = jnp.dot(keys[source], q[k], preferred_element_type=jnp.float32)
        alphas = []
        for k in range(kvl):
            for tile in range(lanes_q // 128):
                at = pl.ds(tile * 128, 128)
                xs = []
                for b in range(nq):
                    x = s_ref[k, b * SEL_BLOCK : (b + 1) * SEL_BLOCK, at]
                    x = x + bias[source, b : b + 1, at]
                    if first:
                        col = lax.broadcasted_iota(jnp.int32, (SEL_BLOCK, 128), 1)
                        row = lax.broadcasted_iota(jnp.int32, (SEL_BLOCK, 128), 0)
                        seen = row + b * SEL_BLOCK <= col + (tile * 128) % rows
                        x = jnp.where(seen, x, NEGATIVE)
                    xs.append(x.reshape(SEL_BLOCK // 8, 8, 128))
                top = functools.reduce(jnp.maximum, [jnp.max(x, axis=0) for x in xs])
                peak = jnp.max(top, axis=0, keepdims=True)
                if not first:
                    before = m_ref[k, 0:1, at]
                    peak = jnp.maximum(before, peak)
                    alphas.append(jnp.exp(before - peak))
                total = None
                for b in range(nq):
                    p = jnp.exp(xs[b] - peak)
                    part = jnp.sum(p, axis=0)
                    total = part if total is None else total + part
                    p_ref[k, b * SEL_BLOCK : (b + 1) * SEL_BLOCK, at] = p.reshape(
                        SEL_BLOCK, 128
                    ).astype(jnp.bfloat16)
                if not first:
                    total = total + l_ref[k, :, at] * alphas[-1]
                m_ref[k, 0:1, at] = peak
                l_ref[k, :, at] = total
        return alphas

    def gather(source, alphas):
        for k in range(kvl):
            got = jnp.dot(
                vals[source, k * hs : (k + 1) * hs, :],
                p_ref[k],
                preferred_element_type=jnp.float32,
            )
            if alphas:
                tiles = lanes_q // 128
                alpha = jnp.concatenate(alphas[k * tiles : (k + 1) * tiles], axis=1)
                got = got + acc_ref[k] * alpha
            acc_ref[k] = got

    gather(me, weigh(me, True))

    @pl.when(core == 1)
    def _():
        across(me - 1, 0).wait_recv()
        alphas = weigh(me - 1, False)
        across(me - 1, 1).wait_recv()
        gather(me - 1, alphas)
        across(me - 1, 2).wait_recv()

    def step(s, carry):
        mine = me - 2 * s
        other = mate - 2 * s

        def take(part):
            upward(mine, part).wait_recv()

            @pl.when(has_up)
            def _():
                upward(mine, part).start()

            across(mine, part).start()

        take(0)
        alphas = weigh(mine, False)
        take(1)
        gather(mine, alphas)
        across(other, 0).wait_recv()
        alphas = weigh(other, False)
        take(2)
        across(other, 1).wait_recv()
        gather(other, alphas)
        across(other, 2).wait_recv()
        return carry

    lax.fori_loop(1, z + 1, step, 0)

    cols = n * cmp_rows
    small = summ[...].reshape(cols, 2 * kcols)
    small_keys = small[:, :kcols].astype(jnp.bfloat16)
    small_vals = small.T[kcols:, :].astype(jnp.bfloat16)
    col = lax.broadcasted_iota(jnp.int32, (cols, rows), 0)
    row = lax.broadcasted_iota(jnp.int32, (cols, rows), 1)
    seen = col * CMP_LEN + (CMP_LEN - 1) <= row + me * rows
    mixed = []
    for k in range(kvl):
        s = jnp.dot(small_keys, q[k], preferred_element_type=jnp.float32)
        sel = acc_ref[k] / jnp.sum(l_ref[k], axis=0, keepdims=True)
        for g in range(group):
            cut = slice(g * rows, (g + 1) * rows)
            x = jnp.where(seen, s[:, cut], NEGATIVE)
            peak = jnp.max(x, axis=0, keepdims=True)
            w = jnp.where(seen, jnp.exp(x - peak), 0.0)
            total = jnp.maximum(jnp.sum(w, axis=0, keepdims=True), 1.0)
            comp = jnp.dot(
                small_vals[k * hs : (k + 1) * hs, :],
                w.astype(jnp.bfloat16),
                preferred_element_type=jnp.float32,
            )
            h = k * group + g
            mixed.append(
                gates[0, h : h + 1, :] / total * comp + gates[1, h : h + 1, :] * sel[:, cut]
            )
    mix[tp] = jnp.concatenate(mixed, axis=0).T.astype(jnp.bfloat16)

    def swap(ref, d, source, kind):
        return pltpu.make_async_remote_copy(
            src_ref=ref.at[source],
            dst_ref=ref.at[source],
            send_sem=tp_send.at[kind, d],
            recv_sem=tp_recv.at[kind, source],
            device_id={"tp": lax.rem(tp + d, tps)},
            device_id_type=MESH,
        )

    for d in range(1, tps):
        swap(mix, d, tp, 0).start()
    loads[7].wait()
    for d in range(1, tps):
        swap(mix, d, lax.rem(tp + d, tps), 0).wait_recv()
    proj = jnp.dot(mix[0], ow[:qcols, :], preferred_element_type=jnp.float32)
    for t in range(1, tps):
        proj = proj + jnp.dot(
            mix[t], ow[t * qcols : (t + 1) * qcols, :], preferred_element_type=jnp.float32
        )
    lanes = proj[:, :128] * proj[:, :128]
    for i in range(1, proj.shape[1] // 128):
        tile = proj[:, i * 128 : (i + 1) * 128]
        lanes = lanes + tile * tile
    sq[tp] = jnp.sum(lanes.T.reshape(16, 8, rows), axis=0)
    for d in range(1, tps):
        swap(sq, d, tp, 1).start()

    for part in range(parts):
        @pl.when(has_up)
        def _():
            upward(me, part).wait_send()

        @pl.when(core == 0)
        def _():
            across(me, part).wait_send()

    def drain(s, carry):
        mine = me - 2 * s
        for part in range(parts):
            @pl.when(has_up)
            def _():
                upward(mine, part).wait_send()

            across(mine, part).wait_send()
        return carry

    lax.fori_loop(1, z + 1, drain, 0)
    for d in range(1, tps):
        swap(sq, d, lax.rem(tp + d, tps), 1).wait_recv()
    squares = jnp.sum(jnp.sum(sq[...], axis=0), axis=0, keepdims=True)
    factor = lax.rsqrt(squares / total_cols + EPSILON)
    column = jnp.broadcast_to(factor, (128, rows)).T
    width_out = out_ref.shape[1]
    gain = gain_ref[:, :width_out].astype(jnp.float32)
    for t in range(1, tps):
        gain = jnp.where(
            tp == t, gain_ref[:, t * width_out : (t + 1) * width_out].astype(jnp.float32), gain
        )
    for i in range(width_out // 128):
        at = slice(i * 128, (i + 1) * 128)
        out_ref[:, at] = (proj[:, at] * column * gain[:, at]).astype(out_ref.dtype)
    for d in range(1, tps):
        swap(mix, d, tp, 0).wait_send()
        swap(sq, d, tp, 1).wait_send()


def body(
    n,
    tps,
    tokens,
    query_weight,
    key_weight,
    value_weight,
    gate_weight,
    squeeze_key,
    squeeze_value,
    out_weight,
    out_gain,
    chosen,
):
    rows, width = tokens.shape
    hs = squeeze_key.shape[1]
    kvl = key_weight.shape[1] // hs
    qcols = query_weight.shape[1]
    group = qcols // hs // kvl
    cols = out_weight.shape[1]
    total_cols = out_gain.shape[0]
    lanes_q = group * rows
    cmp_rows = rows // CMP_LEN
    dims = (rows, width, hs, kvl, group, total_cols, tps)
    kcols = kvl * hs
    joint = kcols % 128 == 0
    spare = (8, 128) if joint else (width, kcols)
    any_spec = pl.BlockSpec(memory_space=pl.ANY)
    vmem = pl.BlockSpec(memory_space=pltpu.VMEM)
    bf, f32 = jnp.bfloat16, jnp.float32
    dma = pltpu.SemaphoreType.DMA
    return pl.pallas_call(
        functools.partial(kernel, n, dims),
        out_shape=jax.ShapeDtypeStruct((rows, cols), bf),
        in_specs=[vmem] * 2 + [any_spec] * 8,
        out_specs=vmem,
        scratch_shapes=[
            pltpu.VMEM((rows, width), bf),
            pltpu.VMEM((width, qcols + 2 * kcols if joint else qcols), bf),
            pltpu.VMEM(spare, bf),
            pltpu.VMEM(spare, bf),
            pltpu.VMEM((gate_weight.shape[0] * gate_weight.shape[2], width), bf),
            pltpu.VMEM(squeeze_key.shape[::-1], bf),
            pltpu.VMEM(squeeze_value.shape[::-1], bf),
            pltpu.VMEM(out_weight.shape, bf),
            pltpu.VMEM((n, rows, kcols), bf),
            pltpu.VMEM((n, kcols, rows), bf),
            pltpu.VMEM((2, rows, max(kcols, 128)), f32),
            pltpu.VMEM((n, cmp_rows, 2 * kcols), f32),
            pltpu.VMEM((n, 8, lanes_q), f32),
            pltpu.VMEM((kvl, kcols, lanes_q), bf),
            pltpu.VMEM((2, 8, rows), f32),
            pltpu.VMEM((kvl, 8, lanes_q), f32),
            pltpu.VMEM((kvl, 8, lanes_q), f32),
            pltpu.VMEM((kvl, hs, lanes_q), f32),
            pltpu.VMEM((kvl, rows, lanes_q), f32),
            pltpu.VMEM((kvl, rows, lanes_q), bf),
            pltpu.VMEM((tps, rows, qcols), bf),
            pltpu.VMEM((tps, 8, rows), f32),
            dma((8,)),
            dma((n, 3)),
            dma((n // 2, 3)),
            dma((n // 2, 3)),
            dma((2, tps)),
            dma((2, tps)),
        ],
        compiler_params=pltpu.CompilerParams(
            collective_id=0, has_side_effects=True, vmem_limit_bytes=56 * 1024 * 1024
        ),
    )(
        chosen,
        out_gain.reshape(1, -1),
        tokens,
        query_weight,
        key_weight,
        value_weight,
        gate_weight.transpose(0, 2, 1).reshape(-1, width),
        squeeze_key.T,
        squeeze_value.T,
        out_weight,
    )


def solution(mesh):
    in_specs = (
        P(("grp", "kv"), None),
        P(None, "tp"),
        P(None, "tp"),
        P(None, "tp"),
        P(),
        P(),
        P(),
        P(None, "tp"),
        P(),
        P(("grp", "kv"), None),
    )
    return jax.shard_map(
        functools.partial(body, mesh.shape["kv"], mesh.shape["tp"]),
        mesh=mesh,
        in_specs=in_specs,
        out_specs=P(("grp", "kv"), "tp"),
        check_vma=False,
    )
```

```python
import functools

import jax
import jax.numpy as jnp
from jax import lax
from jax.experimental import pallas as pl
from jax.experimental.pallas import tpu as pltpu
from jax.sharding import PartitionSpec as P

CMP_LEN = 32
SEL_BLOCK = 64
NEGATIVE = -1e30
EPSILON = 1e-06
MESH = pl.DeviceIdType.MESH
NT = (((1,), (1,)), ((), ()))


def kernel(
    n,
    dims,
    chosen_ref,
    tok_hbm,
    qw_hbm,
    kw_hbm,
    vw_hbm,
    gw_hbm,
    sqk_hbm,
    sqv_hbm,
    ow_hbm,
    gain_hbm,
    out_ref,
    tok,
    weights,
    kw,
    vw,
    gw,
    sqk,
    sqv,
    ow,
    gain_ref,
    keys,
    vals,
    kvf,
    summ,
    bias,
    q,
    gates,
    m_ref,
    l_ref,
    acc_ref,
    s_ref,
    p_ref,
    comp_ref,
    mix,
    sq,
    load_sem,
    recv_sem,
    up_sem,
    across_sem,
    tp_send,
    tp_recv,
):
    rows, width, hs, kvl, group, total_cols, tps = dims
    chips = n // 2
    nq = rows // SEL_BLOCK
    qcols = kvl * group * hs
    cmp_rows = rows // CMP_LEN
    lanes_q = group * rows
    me = lax.axis_index("kv")
    tp = lax.axis_index("tp")
    z = me // 2
    core = me - 2 * z
    mate = 2 * z + 1 - core
    has_up = z < chips - 1
    parts = 3

    kcols = kvl * hs
    joint = kcols % 128 == 0
    if joint:
        kw = weights.at[:, pl.ds(qcols, kcols)]
        vw = weights.at[:, pl.ds(qcols + kcols, kcols)]
    chunks = load_sem.shape[0] // 3 - 2
    step_w = width // chunks
    spots = [pl.ds(c * step_w, step_w) for c in range(chunks)]
    first_loads = []
    for c, spot in enumerate(spots):
        first_loads.append(
            [
                pltpu.make_async_copy(
                    tok_hbm.at[:, spot], tok.at[:, spot], load_sem.at[6 + 3 * c]
                ),
                pltpu.make_async_copy(kw_hbm.at[spot], kw.at[spot], load_sem.at[7 + 3 * c]),
                pltpu.make_async_copy(vw_hbm.at[spot], vw.at[spot], load_sem.at[8 + 3 * c]),
            ]
        )
    for group_loads in first_loads:
        for load in group_loads:
            load.start()
    load_sqk = pltpu.make_async_copy(sqk_hbm, sqk, load_sem.at[0])
    load_sqv = pltpu.make_async_copy(sqv_hbm, sqv, load_sem.at[1])
    load_qw = pltpu.make_async_copy(qw_hbm, weights.at[:, pl.ds(0, qcols)], load_sem.at[2])
    load_gw = pltpu.make_async_copy(gw_hbm, gw, load_sem.at[3])
    load_ow = pltpu.make_async_copy(ow_hbm, ow, load_sem.at[4])
    load_gain = pltpu.make_async_copy(gain_hbm, gain_ref, load_sem.at[5])

    barrier = pltpu.get_barrier_semaphore()
    pl.semaphore_signal(barrier, inc=1, device_id={"kv": mate}, device_id_type=MESH)
    for d in range(1, tps):
        pl.semaphore_signal(
            barrier, inc=1, device_id={"tp": lax.rem(tp + d, tps)}, device_id_type=MESH
        )

    @pl.when(z > 0)
    def _():
        pl.semaphore_signal(barrier, inc=1, device_id={"kv": me - 2}, device_id_type=MESH)

    ids = chosen_ref[...]

    def make_bias(j, carry):
        for b in range(nq):
            hit = jnp.max(jnp.where(ids == j * nq + b, 0.0, NEGATIVE), axis=1, keepdims=True)
            hit = jnp.broadcast_to(hit, (nq, SEL_BLOCK))
            bias[j, b : b + 1, :] = jnp.concatenate(
                [hit[i : i + 1, :] for i in range(nq)] * group, axis=1
            )
        return carry

    lax.fori_loop(0, me + 1, make_bias, 0)

    def clear(j, carry):
        summ[j] = jnp.zeros((cmp_rows, 2 * kcols), jnp.float32)
        return carry

    lax.fori_loop(me + 1, n, clear, 0)

    totals = [None, None]
    for c, spot in enumerate(spots):
        for load in first_loads[c]:
            load.wait()
        if c == chunks - 1:
            for load in (load_sqk, load_sqv, load_qw, load_gw, load_ow, load_gain):
                load.start()
        piece_tok = tok[:, spot]
        if joint:
            got = jnp.dot(
                piece_tok,
                weights[spot, qcols : qcols + 2 * kcols],
                preferred_element_type=jnp.float32,
            )
            got = [got[:, :kcols], got[:, kcols:]]
        else:
            got = [
                jnp.dot(piece_tok, w[spot, :], preferred_element_type=jnp.float32)
                for w in (kw, vw)
            ]
        totals = [g if t is None else t + g for t, g in zip(totals, got)]
    sides = totals
    sides = [side.astype(jnp.bfloat16).astype(jnp.float32) for side in sides]
    for i, side in enumerate(sides):
        if not joint:
            side = jnp.concatenate([side, jnp.zeros((rows, 128 - kcols), jnp.float32)], axis=1)
        kvf[i] = side
    keys[me] = sides[0].astype(jnp.bfloat16)
    vals[me] = sides[1].T.astype(jnp.bfloat16)

    def piece(source, part):
        return (keys, summ, vals)[part].at[source]

    def upward(source, part):
        return pltpu.make_async_remote_copy(
            src_ref=piece(source, part),
            dst_ref=piece(source, part),
            send_sem=up_sem.at[source // 2, part],
            recv_sem=recv_sem.at[source, part],
            device_id={"kv": me + 2},
            device_id_type=MESH,
        )

    def across(source, part):
        return pltpu.make_async_remote_copy(
            src_ref=piece(source, part),
            dst_ref=piece(source, part),
            send_sem=across_sem.at[source // 2, part],
            recv_sem=recv_sem.at[source, part],
            device_id={"kv": mate},
            device_id_type=MESH,
        )

    pl.semaphore_wait(barrier, tps + jnp.minimum(chips - 1 - z, 1))

    def send_own(part):
        @pl.when(has_up)
        def _():
            upward(me, part).start()

        @pl.when(core == 0)
        def _():
            across(me, part).start()

    send_own(0)

    load_sqk.wait()
    load_sqv.wait()
    squeezed = []
    for side, weight in ((0, sqk), (1, sqv)):
        tiles = []
        for p in range(0, CMP_LEN, 2):
            a = kvf[side, pl.ds(p, cmp_rows, stride=CMP_LEN), :]
            b = kvf[side, pl.ds(p + 1, cmp_rows, stride=CMP_LEN), :]
            heads = [
                jnp.concatenate([x[:, k * hs : (k + 1) * hs] for x in (a, b)], axis=1)
                for k in range(kvl)
            ]
            tiles.append(jnp.concatenate(heads, axis=0))
        flat = jnp.concatenate(tiles, axis=1).astype(jnp.bfloat16)
        squeezed.append(
            lax.dot_general(flat, weight[...], NT, preferred_element_type=jnp.float32)
            .astype(jnp.bfloat16)
            .astype(jnp.float32)
        )
    summ[me] = jnp.concatenate(
        [
            half[k * cmp_rows : (k + 1) * cmp_rows]
            for half in squeezed
            for k in range(kvl)
        ],
        axis=1,
    )
    send_own(1)
    send_own(2)

    load_qw.wait()
    scale = hs ** (-0.5)
    queries = (
        jnp.dot(tok[...], weights[:, :qcols], preferred_element_type=jnp.float32)
        .astype(jnp.bfloat16)
        .astype(jnp.float32)
        * scale
    )
    turned = queries.T.astype(jnp.bfloat16)
    for k in range(kvl):
        q[k] = jnp.zeros((kcols, lanes_q), jnp.bfloat16)
        for g in range(group):
            h = k * group + g
            q[k, k * hs : (k + 1) * hs, g * rows : (g + 1) * rows] = turned[
                h * hs : (h + 1) * hs, :
            ]
    load_gw.wait()
    hl = kvl * group
    every = jax.nn.sigmoid(
        lax.dot_general(gw[...], tok[...], NT, preferred_element_type=jnp.float32)
    )
    for branch in range(2):
        base = branch * tps * hl
        mine = every[base : base + hl, :]
        for t in range(1, tps):
            mine = jnp.where(tp == t, every[base + t * hl : base + (t + 1) * hl, :], mine)
        gates[branch, 0:hl, :] = mine

    def weigh(source, first, slot=0):
        for k in range(kvl):
            s_ref[k] = jnp.dot(keys[source], q[k], preferred_element_type=jnp.float32)
        alphas = []
        for k in range(kvl):
            for tile in range(lanes_q // 128):
                at = pl.ds(tile * 128, 128)
                xs = []
                for b in range(nq):
                    x = s_ref[k, b * SEL_BLOCK : (b + 1) * SEL_BLOCK, at]
                    x = x + bias[source, b : b + 1, at]
                    if first:
                        col = lax.broadcasted_iota(jnp.int32, (SEL_BLOCK, 128), 1)
                        row = lax.broadcasted_iota(jnp.int32, (SEL_BLOCK, 128), 0)
                        seen = row + b * SEL_BLOCK <= col + (tile * 128) % rows
                        x = jnp.where(seen, x, NEGATIVE)
                    xs.append(x.reshape(SEL_BLOCK // 8, 8, 128))
                top = functools.reduce(jnp.maximum, [jnp.max(x, axis=0) for x in xs])
                peak = jnp.max(top, axis=0, keepdims=True)
                if not first:
                    before = m_ref[k, 0:1, at]
                    peak = jnp.maximum(before, peak)
                    alphas.append(jnp.exp(before - peak))
                total = None
                for b in range(nq):
                    p = jnp.exp(xs[b] - peak)
                    part = jnp.sum(p, axis=0)
                    total = part if total is None else total + part
                    p_ref[slot, k, b * SEL_BLOCK : (b + 1) * SEL_BLOCK, at] = p.reshape(
                        SEL_BLOCK, 128
                    ).astype(jnp.bfloat16)
                if not first:
                    total = total + l_ref[k, :, at] * alphas[-1]
                m_ref[k, 0:1, at] = peak
                l_ref[k, :, at] = total
        return alphas

    def gather(source, alphas, slot=0):
        for k in range(kvl):
            got = jnp.dot(
                vals[source, k * hs : (k + 1) * hs, :],
                p_ref[slot, k],
                preferred_element_type=jnp.float32,
            )
            if alphas:
                tiles = lanes_q // 128
                alpha = jnp.concatenate(alphas[k * tiles : (k + 1) * tiles], axis=1)
                got = got + acc_ref[k] * alpha
            acc_ref[k] = got

    gather(me, weigh(me, True))

    cols = n * cmp_rows

    def compress():
        small = summ[...].reshape(cols, 2 * kcols)
        small_keys = small[:, :kcols].astype(jnp.bfloat16)
        small_vals = small.T[kcols:, :].astype(jnp.bfloat16)
        col = lax.broadcasted_iota(jnp.int32, (cols, rows), 0)
        row = lax.broadcasted_iota(jnp.int32, (cols, rows), 1)
        seen = col * CMP_LEN + (CMP_LEN - 1) <= row + me * rows
        for k in range(kvl):
            s = jnp.dot(small_keys, q[k], preferred_element_type=jnp.float32)
            for g in range(group):
                x = jnp.where(seen, s[:, g * rows : (g + 1) * rows], NEGATIVE)
                peak = jnp.max(x, axis=0, keepdims=True)
                w = jnp.where(seen, jnp.exp(x - peak), 0.0)
                total = jnp.maximum(jnp.sum(w, axis=0, keepdims=True), 1.0)
                comp = jnp.dot(
                    small_vals[k * hs : (k + 1) * hs, :],
                    w.astype(jnp.bfloat16),
                    preferred_element_type=jnp.float32,
                )
                h = k * group + g
                comp_ref[k, :, g * rows : (g + 1) * rows] = comp * (
                    gates[0, h : h + 1, :] / total
                )

    @pl.when(core == 1)
    def _():
        across(me - 1, 0).wait_recv()
        alphas = weigh(me - 1, False)
        across(me - 1, 1).wait_recv()
        across(me - 1, 2).wait_recv()
        gather(me - 1, alphas)

    @pl.when(z == 0)
    def _():
        compress()

    def step(s, carry):
        mine = me - 2 * s
        other = mate - 2 * s

        def take(part):
            upward(mine, part).wait_recv()

            @pl.when(has_up)
            def _():
                upward(mine, part).start()

            across(mine, part).start()

        take(0)
        alphas = weigh(mine, False)
        take(1)
        across(other, 0).wait_recv()
        alphas_other = weigh(other, False, 1)
        across(other, 1).wait_recv()

        @pl.when(s == z)
        def _():
            compress()

        take(2)
        gather(mine, alphas)
        across(other, 2).wait_recv()
        gather(other, alphas_other, 1)
        return carry

    lax.fori_loop(1, z + 1, step, 0)

    def swap(ref, d, source, kind):
        return pltpu.make_async_remote_copy(
            src_ref=ref.at[source],
            dst_ref=ref.at[source],
            send_sem=tp_send.at[kind, d],
            recv_sem=tp_recv.at[kind, source // (kvl if kind < kvl else 1)],
            device_id={"tp": lax.rem(tp + d, tps)},
            device_id_type=MESH,
        )

    for k in range(kvl):
        sel = acc_ref[k] / jnp.sum(l_ref[k], axis=0, keepdims=True)
        mixed = []
        for g in range(group):
            h = k * group + g
            at = slice(g * rows, (g + 1) * rows)
            mixed.append(comp_ref[k, :, at] + gates[1, h : h + 1, :] * sel[:, at])
        mix[tp * kvl + k] = jnp.concatenate(mixed, axis=0).T.astype(jnp.bfloat16)
        for d in range(1, tps):
            swap(mix, d, tp * kvl + k, k).start()
    load_ow.wait()
    load_gain.wait()
    tall = group * hs

    def product(t, k):
        at = pl.ds(pl.multiple_of((t * kvl + k) * tall, tall), tall)
        return jnp.dot(mix[t * kvl + k], ow[at, :], preferred_element_type=jnp.float32)

    proj = product(tp, 0)
    for k in range(1, kvl):
        proj = proj + product(tp, k)
    for k in range(kvl):
        for d in range(1, tps):
            t = lax.rem(tp + d, tps)
            swap(mix, d, t * kvl + k, k).wait_recv()
            proj = proj + product(t, k)
    lanes = proj[:, :128] * proj[:, :128]
    for i in range(1, proj.shape[1] // 128):
        tile = proj[:, i * 128 : (i + 1) * 128]
        lanes = lanes + tile * tile
    sq[tp] = jnp.sum(lanes.T.reshape(16, 8, rows), axis=0)
    for d in range(1, tps):
        swap(sq, d, tp, kvl).start()

    for part in range(parts):
        @pl.when(has_up)
        def _():
            upward(me, part).wait_send()

        @pl.when(core == 0)
        def _():
            across(me, part).wait_send()

    def drain(s, carry):
        mine = me - 2 * s
        for part in range(parts):
            @pl.when(has_up)
            def _():
                upward(mine, part).wait_send()

            across(mine, part).wait_send()
        return carry

    lax.fori_loop(1, z + 1, drain, 0)
    for d in range(1, tps):
        swap(sq, d, lax.rem(tp + d, tps), kvl).wait_recv()
    squares = jnp.sum(jnp.sum(sq[...], axis=0), axis=0, keepdims=True)
    factor = lax.rsqrt(squares / total_cols + EPSILON)
    column = jnp.broadcast_to(factor, (128, rows)).T
    width_out = out_ref.shape[1]
    gain_all = gain_ref[...].astype(jnp.float32).reshape(1, total_cols)
    gain = gain_all[:, :width_out]
    for t in range(1, tps):
        gain = jnp.where(tp == t, gain_all[:, t * width_out : (t + 1) * width_out], gain)
    for i in range(width_out // 128):
        at = slice(i * 128, (i + 1) * 128)
        out_ref[:, at] = (proj[:, at] * column * gain[:, at]).astype(out_ref.dtype)
    for d in range(1, tps):
        for k in range(kvl):
            swap(mix, d, tp * kvl + k, k).wait_send()
        swap(sq, d, tp, kvl).wait_send()


def body(
    n,
    tps,
    tokens,
    query_weight,
    key_weight,
    value_weight,
    gate_weight,
    squeeze_key,
    squeeze_value,
    out_weight,
    out_gain,
    chosen,
):
    rows, width = tokens.shape
    hs = squeeze_key.shape[1]
    kvl = key_weight.shape[1] // hs
    qcols = query_weight.shape[1]
    group = qcols // hs // kvl
    cols = out_weight.shape[1]
    total_cols = out_gain.shape[0]
    lanes_q = group * rows
    cmp_rows = rows // CMP_LEN
    dims = (rows, width, hs, kvl, group, total_cols, tps)
    kcols = kvl * hs
    joint = kcols % 128 == 0
    spare = (8, 128) if joint else (width, kcols)
    any_spec = pl.BlockSpec(memory_space=pltpu.HBM)
    vmem = pl.BlockSpec(memory_space=pltpu.VMEM)
    bf, f32 = jnp.bfloat16, jnp.float32
    dma = pltpu.SemaphoreType.DMA
    return pl.pallas_call(
        functools.partial(kernel, n, dims),
        out_shape=jax.ShapeDtypeStruct((rows, cols), bf),
        in_specs=[vmem] + [any_spec] * 9,
        out_specs=vmem,
        scratch_shapes=[
            pltpu.VMEM((rows, width), bf),
            pltpu.VMEM((width, qcols + 2 * kcols if joint else qcols), bf),
            pltpu.VMEM(spare, bf),
            pltpu.VMEM(spare, bf),
            pltpu.VMEM((gate_weight.shape[0] * gate_weight.shape[2], width), bf),
            pltpu.VMEM(squeeze_key.shape[::-1], bf),
            pltpu.VMEM(squeeze_value.shape[::-1], bf),
            pltpu.VMEM(out_weight.shape, bf),
            pltpu.VMEM(out_gain.shape, bf),
            pltpu.VMEM((n, rows, kcols), bf),
            pltpu.VMEM((n, kcols, rows), bf),
            pltpu.VMEM((2, rows, max(kcols, 128)), f32),
            pltpu.VMEM((n, cmp_rows, 2 * kcols), f32),
            pltpu.VMEM((n, 8, lanes_q), f32),
            pltpu.VMEM((kvl, kcols, lanes_q), bf),
            pltpu.VMEM((2, 8, rows), f32),
            pltpu.VMEM((kvl, 8, lanes_q), f32),
            pltpu.VMEM((kvl, 8, lanes_q), f32),
            pltpu.VMEM((kvl, hs, lanes_q), f32),
            pltpu.VMEM((kvl, rows, lanes_q), f32),
            pltpu.VMEM((2, kvl, rows, lanes_q), bf),
            pltpu.VMEM((kvl, hs, lanes_q), f32),
            pltpu.VMEM((tps * kvl, rows, group * hs), bf),
            pltpu.VMEM((tps, 8, rows), f32),
            dma((18,)),
            dma((n, 3)),
            dma((n // 2, 3)),
            dma((n // 2, 3)),
            dma((kvl + 1, tps)),
            dma((kvl + 1, tps)),
        ],
        compiler_params=pltpu.CompilerParams(
            collective_id=0, has_side_effects=True, vmem_limit_bytes=28 * 1024 * 1024
        ),
    )(
        chosen,
        tokens,
        query_weight,
        key_weight,
        value_weight,
        gate_weight.transpose(0, 2, 1).reshape(-1, width),
        squeeze_key.T,
        squeeze_value.T,
        out_weight,
        out_gain,
    )


def solution(mesh):
    in_specs = (
        P(("grp", "kv"), None),
        P(None, "tp"),
        P(None, "tp"),
        P(None, "tp"),
        P(),
        P(),
        P(),
        P(None, "tp"),
        P(),
        P(("grp", "kv"), None),
    )
    return jax.shard_map(
        functools.partial(body, mesh.shape["kv"], mesh.shape["tp"]),
        mesh=mesh,
        in_specs=in_specs,
        out_specs=P(("grp", "kv"), "tp"),
        check_vma=False,
    )
```

```python
import functools

import jax
import jax.numpy as jnp
from jax import lax
from jax.experimental import pallas as pl
from jax.experimental.pallas import tpu as pltpu
from jax.sharding import PartitionSpec as P

CMP_LEN = 32
SEL_BLOCK = 64
NEGATIVE = -1e30
EPSILON = 1e-06
MESH = pl.DeviceIdType.MESH
NT = (((1,), (1,)), ((), ()))


def kernel(
    n,
    dims,
    chosen_ref,
    tok_hbm,
    qw_hbm,
    kw_hbm,
    vw_hbm,
    gw_hbm,
    sqk_hbm,
    sqv_hbm,
    ow_hbm,
    gain_hbm,
    out_ref,
    tok,
    weights,
    kw,
    vw,
    gw,
    sqk,
    sqv,
    ow,
    gain_ref,
    keys,
    vals,
    kvf,
    summ,
    bias,
    q,
    gates,
    m_ref,
    l_ref,
    acc_ref,
    s_ref,
    p_ref,
    comp_ref,
    mix,
    sq,
    load_sem,
    recv_sem,
    up_sem,
    across_sem,
    tp_send,
    tp_recv,
):
    rows, width, hs, kvl, group, total_cols, tps = dims
    chips = n // 2
    nq = rows // SEL_BLOCK
    qcols = kvl * group * hs
    cmp_rows = rows // CMP_LEN
    lanes_q = group * rows
    me = lax.axis_index("kv")
    tp = lax.axis_index("tp")
    z = me // 2
    core = me - 2 * z
    mate = 2 * z + 1 - core
    has_up = z < chips - 1
    parts = 3

    kcols = kvl * hs
    joint = kcols % 128 == 0
    if joint:
        kw = weights.at[:, pl.ds(qcols, kcols)]
        vw = weights.at[:, pl.ds(qcols + kcols, kcols)]
    chunks = load_sem.shape[0] // 3 - 2
    step_w = width // chunks
    spots = [pl.ds(c * step_w, step_w) for c in range(chunks)]
    first_loads = []
    for c, spot in enumerate(spots):
        first_loads.append(
            [
                pltpu.make_async_copy(
                    tok_hbm.at[:, spot], tok.at[:, spot], load_sem.at[6 + 3 * c]
                ),
                pltpu.make_async_copy(kw_hbm.at[spot], kw.at[spot], load_sem.at[7 + 3 * c]),
                pltpu.make_async_copy(vw_hbm.at[spot], vw.at[spot], load_sem.at[8 + 3 * c]),
            ]
        )
    for group_loads in first_loads:
        for load in group_loads:
            load.start()
    load_sqk = pltpu.make_async_copy(sqk_hbm, sqk, load_sem.at[0])
    load_sqv = pltpu.make_async_copy(sqv_hbm, sqv, load_sem.at[1])
    load_qw = pltpu.make_async_copy(qw_hbm, weights.at[:, pl.ds(0, qcols)], load_sem.at[2])
    load_gw = pltpu.make_async_copy(gw_hbm, gw, load_sem.at[3])
    load_ow = pltpu.make_async_copy(ow_hbm, ow, load_sem.at[4])
    load_gain = pltpu.make_async_copy(gain_hbm, gain_ref, load_sem.at[5])

    barrier = pltpu.get_barrier_semaphore()
    pl.semaphore_signal(barrier, inc=1, device_id={"kv": mate}, device_id_type=MESH)
    for d in range(1, tps):
        pl.semaphore_signal(
            barrier, inc=1, device_id={"tp": lax.rem(tp + d, tps)}, device_id_type=MESH
        )

    @pl.when(z > 0)
    def _():
        pl.semaphore_signal(barrier, inc=1, device_id={"kv": me - 2}, device_id_type=MESH)

    ids = chosen_ref[...]

    def make_bias(j, carry):
        for b in range(nq):
            hit = jnp.max(jnp.where(ids == j * nq + b, 0.0, NEGATIVE), axis=1, keepdims=True)
            hit = jnp.broadcast_to(hit, (nq, SEL_BLOCK))
            bias[j, b : b + 1, :] = jnp.concatenate(
                [hit[i : i + 1, :] for i in range(nq)] * group, axis=1
            )
        return carry

    lax.fori_loop(0, me + 1, make_bias, 0)

    def clear(j, carry):
        summ[j] = jnp.zeros((cmp_rows, 2 * kcols), jnp.float32)
        return carry

    lax.fori_loop(me + 1, n, clear, 0)

    totals = [None, None]
    for c, spot in enumerate(spots):
        for load in first_loads[c]:
            load.wait()
        if c == chunks - 1:
            for load in (load_sqk, load_sqv, load_qw, load_gw, load_ow, load_gain):
                load.start()
        piece_tok = tok[:, spot]
        if joint:
            got = jnp.dot(
                piece_tok,
                weights[spot, qcols : qcols + 2 * kcols],
                preferred_element_type=jnp.float32,
            )
            got = [got[:, :kcols], got[:, kcols:]]
        else:
            got = [
                jnp.dot(piece_tok, w[spot, :], preferred_element_type=jnp.float32)
                for w in (kw, vw)
            ]
        totals = [g if t is None else t + g for t, g in zip(totals, got)]
    sides = totals
    sides = [side.astype(jnp.bfloat16).astype(jnp.float32) for side in sides]
    for i, side in enumerate(sides):
        if not joint:
            side = jnp.concatenate([side, jnp.zeros((rows, 128 - kcols), jnp.float32)], axis=1)
        kvf[i] = side
    keys[me] = sides[0].astype(jnp.bfloat16)
    vals[me] = sides[1].T.astype(jnp.bfloat16)

    def piece(source, part):
        return (keys, summ, vals)[part].at[source]

    def upward(source, part):
        return pltpu.make_async_remote_copy(
            src_ref=piece(source, part),
            dst_ref=piece(source, part),
            send_sem=up_sem.at[source // 2, part],
            recv_sem=recv_sem.at[source, part],
            device_id={"kv": me + 2},
            device_id_type=MESH,
        )

    def across(source, part):
        return pltpu.make_async_remote_copy(
            src_ref=piece(source, part),
            dst_ref=piece(source, part),
            send_sem=across_sem.at[source // 2, part],
            recv_sem=recv_sem.at[source, part],
            device_id={"kv": mate},
            device_id_type=MESH,
        )

    pl.semaphore_wait(barrier, tps + jnp.minimum(chips - 1 - z, 1))

    def send_own(part):
        @pl.when(has_up)
        def _():
            upward(me, part).start()

        @pl.when(core == 0)
        def _():
            across(me, part).start()

    send_own(0)

    load_sqk.wait()
    load_sqv.wait()
    squeezed = []
    for side, weight in ((0, sqk), (1, sqv)):
        tiles = []
        for p in range(0, CMP_LEN, 2):
            a = kvf[side, pl.ds(p, cmp_rows, stride=CMP_LEN), :]
            b = kvf[side, pl.ds(p + 1, cmp_rows, stride=CMP_LEN), :]
            heads = [
                jnp.concatenate([x[:, k * hs : (k + 1) * hs] for x in (a, b)], axis=1)
                for k in range(kvl)
            ]
            tiles.append(jnp.concatenate(heads, axis=0))
        flat = jnp.concatenate(tiles, axis=1).astype(jnp.bfloat16)
        squeezed.append(
            lax.dot_general(flat, weight[...], NT, preferred_element_type=jnp.float32)
            .astype(jnp.bfloat16)
            .astype(jnp.float32)
        )
    summ[me] = jnp.concatenate(
        [
            half[k * cmp_rows : (k + 1) * cmp_rows]
            for half in squeezed
            for k in range(kvl)
        ],
        axis=1,
    )
    send_own(1)
    send_own(2)

    load_qw.wait()
    scale = hs ** (-0.5)
    queries = (
        jnp.dot(tok[...], weights[:, :qcols], preferred_element_type=jnp.float32)
        .astype(jnp.bfloat16)
        .astype(jnp.float32)
        * scale
    )
    turned = queries.T.astype(jnp.bfloat16)
    for k in range(kvl):
        q[k] = jnp.zeros((kcols, lanes_q), jnp.bfloat16)
        for g in range(group):
            h = k * group + g
            q[k, k * hs : (k + 1) * hs, g * rows : (g + 1) * rows] = turned[
                h * hs : (h + 1) * hs, :
            ]
    load_gw.wait()
    hl = kvl * group
    every = jax.nn.sigmoid(
        lax.dot_general(gw[...], tok[...], NT, preferred_element_type=jnp.float32)
    )
    for branch in range(2):
        base = branch * tps * hl
        mine = every[base : base + hl, :]
        for t in range(1, tps):
            mine = jnp.where(tp == t, every[base + t * hl : base + (t + 1) * hl, :], mine)
        gates[branch, 0:hl, :] = mine

    def weigh(source, first, slot=0):
        for k in range(kvl):
            s_ref[k] = jnp.dot(keys[source], q[k], preferred_element_type=jnp.float32)
        alphas = []
        for k in range(kvl):
            for tile in range(lanes_q // 128):
                at = pl.ds(tile * 128, 128)
                xs = []
                for b in range(nq):
                    x = s_ref[k, b * SEL_BLOCK : (b + 1) * SEL_BLOCK, at]
                    x = x + bias[source, b : b + 1, at]
                    if first:
                        col = lax.broadcasted_iota(jnp.int32, (SEL_BLOCK, 128), 1)
                        row = lax.broadcasted_iota(jnp.int32, (SEL_BLOCK, 128), 0)
                        seen = row + b * SEL_BLOCK <= col + (tile * 128) % rows
                        x = jnp.where(seen, x, NEGATIVE)
                    xs.append(x.reshape(SEL_BLOCK // 8, 8, 128))
                top = functools.reduce(jnp.maximum, [jnp.max(x, axis=0) for x in xs])
                peak = jnp.max(top, axis=0, keepdims=True)
                if not first:
                    before = m_ref[k, 0:1, at]
                    peak = jnp.maximum(before, peak)
                    alphas.append(jnp.exp(before - peak))
                total = None
                for b in range(nq):
                    p = jnp.exp(xs[b] - peak)
                    part = jnp.sum(p, axis=0)
                    total = part if total is None else total + part
                    p_ref[slot, k, b * SEL_BLOCK : (b + 1) * SEL_BLOCK, at] = p.reshape(
                        SEL_BLOCK, 128
                    ).astype(jnp.bfloat16)
                if not first:
                    total = total + l_ref[k, :, at] * alphas[-1]
                m_ref[k, 0:1, at] = peak
                l_ref[k, :, at] = total
        return alphas

    def gather(source, alphas, slot=0):
        for k in range(kvl):
            got = jnp.dot(
                vals[source, k * hs : (k + 1) * hs, :],
                p_ref[slot, k],
                preferred_element_type=jnp.float32,
            )
            if alphas:
                tiles = lanes_q // 128
                alpha = jnp.concatenate(alphas[k * tiles : (k + 1) * tiles], axis=1)
                got = got + acc_ref[k] * alpha
            acc_ref[k] = got

    gather(me, weigh(me, True))

    cols = n * cmp_rows

    def compress():
        small = summ[...].reshape(cols, 2 * kcols)
        small_keys = small[:, :kcols].astype(jnp.bfloat16)
        small_vals = small.T[kcols:, :].astype(jnp.bfloat16)
        col = lax.broadcasted_iota(jnp.int32, (cols, rows), 0)
        row = lax.broadcasted_iota(jnp.int32, (cols, rows), 1)
        seen = col * CMP_LEN + (CMP_LEN - 1) <= row + me * rows
        for k in range(kvl):
            s = jnp.dot(small_keys, q[k], preferred_element_type=jnp.float32)
            for g in range(group):
                x = jnp.where(seen, s[:, g * rows : (g + 1) * rows], NEGATIVE)
                peak = jnp.max(x, axis=0, keepdims=True)
                w = jnp.where(seen, jnp.exp(x - peak), 0.0)
                total = jnp.maximum(jnp.sum(w, axis=0, keepdims=True), 1.0)
                comp = jnp.dot(
                    small_vals[k * hs : (k + 1) * hs, :],
                    w.astype(jnp.bfloat16),
                    preferred_element_type=jnp.float32,
                )
                h = k * group + g
                comp_ref[k, :, g * rows : (g + 1) * rows] = comp * (
                    gates[0, h : h + 1, :] / total
                )

    @pl.when(core == 1)
    def _():
        across(me - 1, 0).wait_recv()
        alphas = weigh(me - 1, False)
        across(me - 1, 1).wait_recv()
        across(me - 1, 2).wait_recv()
        gather(me - 1, alphas)

    @pl.when(z == 0)
    def _():
        compress()

    def step(s, carry):
        mine = me - 2 * s
        other = mate - 2 * s

        def take(part):
            upward(mine, part).wait_recv()

            @pl.when(has_up)
            def _():
                upward(mine, part).start()

            across(mine, part).start()

        take(0)
        alphas = weigh(mine, False)
        take(1)
        across(other, 0).wait_recv()
        alphas_other = weigh(other, False, 1)
        across(other, 1).wait_recv()

        @pl.when(s == z)
        def _():
            compress()

        take(2)
        gather(mine, alphas)
        across(other, 2).wait_recv()
        gather(other, alphas_other, 1)
        return carry

    lax.fori_loop(1, z + 1, step, 0)

    def swap(ref, d, source, kind):
        return pltpu.make_async_remote_copy(
            src_ref=ref.at[source],
            dst_ref=ref.at[source],
            send_sem=tp_send.at[kind, d],
            recv_sem=tp_recv.at[kind, source // (kvl if kind < kvl else 1)],
            device_id={"tp": lax.rem(tp + d, tps)},
            device_id_type=MESH,
        )

    for k in range(kvl):
        sel = acc_ref[k] / jnp.sum(l_ref[k], axis=0, keepdims=True)
        mixed = []
        for g in range(group):
            h = k * group + g
            at = slice(g * rows, (g + 1) * rows)
            mixed.append(comp_ref[k, :, at] + gates[1, h : h + 1, :] * sel[:, at])
        mix[tp * kvl + k] = jnp.concatenate(mixed, axis=0).T.astype(jnp.bfloat16)
        for d in range(1, tps):
            swap(mix, d, tp * kvl + k, k).start()
    load_ow.wait()
    load_gain.wait()
    tall = group * hs

    def product(t, k):
        at = pl.ds(pl.multiple_of((t * kvl + k) * tall, tall), tall)
        return jnp.dot(mix[t * kvl + k], ow[at, :], preferred_element_type=jnp.float32)

    proj = product(tp, 0)
    for k in range(1, kvl):
        proj = proj + product(tp, k)
    for k in range(kvl):
        for d in range(1, tps):
            t = lax.rem(tp + d, tps)
            swap(mix, d, t * kvl + k, k).wait_recv()
            proj = proj + product(t, k)
    lanes = proj[:, :128] * proj[:, :128]
    for i in range(1, proj.shape[1] // 128):
        tile = proj[:, i * 128 : (i + 1) * 128]
        lanes = lanes + tile * tile
    sq[tp] = jnp.sum(lanes.T.reshape(16, 8, rows), axis=0)
    for d in range(1, tps):
        swap(sq, d, tp, kvl).start()

    for part in range(parts):
        @pl.when(has_up)
        def _():
            upward(me, part).wait_send()

        @pl.when(core == 0)
        def _():
            across(me, part).wait_send()

    def drain(s, carry):
        mine = me - 2 * s
        for part in range(parts):
            @pl.when(has_up)
            def _():
                upward(mine, part).wait_send()

            across(mine, part).wait_send()
        return carry

    lax.fori_loop(1, z + 1, drain, 0)
    for d in range(1, tps):
        swap(sq, d, lax.rem(tp + d, tps), kvl).wait_recv()
    squares = jnp.sum(jnp.sum(sq[...], axis=0), axis=0, keepdims=True)
    factor = lax.rsqrt(squares / total_cols + EPSILON)
    column = jnp.broadcast_to(factor, (128, rows)).T
    width_out = out_ref.shape[1]
    gain_all = gain_ref[...].astype(jnp.float32).reshape(1, total_cols)
    gain = gain_all[:, :width_out]
    for t in range(1, tps):
        gain = jnp.where(tp == t, gain_all[:, t * width_out : (t + 1) * width_out], gain)
    for i in range(width_out // 128):
        at = slice(i * 128, (i + 1) * 128)
        out_ref[:, at] = (proj[:, at] * column * gain[:, at]).astype(out_ref.dtype)
    for d in range(1, tps):
        for k in range(kvl):
            swap(mix, d, tp * kvl + k, k).wait_send()
        swap(sq, d, tp, kvl).wait_send()


def body(
    n,
    tps,
    tokens,
    query_weight,
    key_weight,
    value_weight,
    gate_weight,
    squeeze_key,
    squeeze_value,
    out_weight,
    out_gain,
    chosen,
):
    rows, width = tokens.shape
    hs = squeeze_key.shape[1]
    kvl = key_weight.shape[1] // hs
    qcols = query_weight.shape[1]
    group = qcols // hs // kvl
    cols = out_weight.shape[1]
    total_cols = out_gain.shape[0]
    lanes_q = group * rows
    cmp_rows = rows // CMP_LEN
    dims = (rows, width, hs, kvl, group, total_cols, tps)
    kcols = kvl * hs
    joint = kcols % 128 == 0
    spare = (8, 128) if joint else (width, kcols)
    any_spec = pl.BlockSpec(memory_space=pl.ANY)
    vmem = pl.BlockSpec(memory_space=pltpu.VMEM)
    bf, f32 = jnp.bfloat16, jnp.float32
    dma = pltpu.SemaphoreType.DMA
    return pl.pallas_call(
        functools.partial(kernel, n, dims),
        out_shape=jax.ShapeDtypeStruct((rows, cols), bf),
        in_specs=[vmem] + [any_spec] * 9,
        out_specs=vmem,
        scratch_shapes=[
            pltpu.VMEM((rows, width), bf),
            pltpu.VMEM((width, qcols + 2 * kcols if joint else qcols), bf),
            pltpu.VMEM(spare, bf),
            pltpu.VMEM(spare, bf),
            pltpu.VMEM((gate_weight.shape[0] * gate_weight.shape[2], width), bf),
            pltpu.VMEM(squeeze_key.shape[::-1], bf),
            pltpu.VMEM(squeeze_value.shape[::-1], bf),
            pltpu.VMEM(out_weight.shape, bf),
            pltpu.VMEM(out_gain.shape, bf),
            pltpu.VMEM((n, rows, kcols), bf),
            pltpu.VMEM((n, kcols, rows), bf),
            pltpu.VMEM((2, rows, max(kcols, 128)), f32),
            pltpu.VMEM((n, cmp_rows, 2 * kcols), f32),
            pltpu.VMEM((n, 8, lanes_q), f32),
            pltpu.VMEM((kvl, kcols, lanes_q), bf),
            pltpu.VMEM((2, 8, rows), f32),
            pltpu.VMEM((kvl, 8, lanes_q), f32),
            pltpu.VMEM((kvl, 8, lanes_q), f32),
            pltpu.VMEM((kvl, hs, lanes_q), f32),
            pltpu.VMEM((kvl, rows, lanes_q), f32),
            pltpu.VMEM((2, kvl, rows, lanes_q), bf),
            pltpu.VMEM((kvl, hs, lanes_q), f32),
            pltpu.VMEM((tps * kvl, rows, group * hs), bf),
            pltpu.VMEM((tps, 8, rows), f32),
            dma((18,)),
            dma((n, 3)),
            dma((n // 2, 3)),
            dma((n // 2, 3)),
            dma((kvl + 1, tps)),
            dma((kvl + 1, tps)),
        ],
        compiler_params=pltpu.CompilerParams(
            collective_id=0, has_side_effects=True, vmem_limit_bytes=56 * 1024 * 1024
        ),
    )(
        chosen,
        tokens,
        query_weight,
        key_weight,
        value_weight,
        gate_weight.transpose(0, 2, 1).reshape(-1, width),
        squeeze_key.T,
        squeeze_value.T,
        out_weight,
        out_gain,
    )


def solution(mesh):
    in_specs = (
        P(("grp", "kv"), None),
        P(None, "tp"),
        P(None, "tp"),
        P(None, "tp"),
        P(),
        P(),
        P(),
        P(None, "tp"),
        P(),
        P(("grp", "kv"), None),
    )
    return jax.shard_map(
        functools.partial(body, mesh.shape["kv"], mesh.shape["tp"]),
        mesh=mesh,
        in_specs=in_specs,
        out_specs=P(("grp", "kv"), "tp"),
        check_vma=False,
    )
```

```python
import functools

import jax
import jax.numpy as jnp
from jax import lax
from jax.experimental import pallas as pl
from jax.experimental.pallas import tpu as pltpu
from jax.sharding import PartitionSpec as P

CMP_LEN = 32
SEL_BLOCK = 64
NEGATIVE = -1e30
EPSILON = 1e-06
MESH = pl.DeviceIdType.MESH
NT = (((1,), (1,)), ((), ()))


def kernel(
    n,
    dims,
    chosen_ref,
    tok_hbm,
    qw_hbm,
    kw_hbm,
    vw_hbm,
    gw_hbm,
    sqk_hbm,
    sqv_hbm,
    ow_hbm,
    gain_hbm,
    out_ref,
    tok,
    weights,
    kw,
    vw,
    gw,
    sqk,
    sqv,
    ow,
    gain_ref,
    keys,
    vals,
    kvf,
    summ,
    bias,
    q,
    gates,
    m_ref,
    l_ref,
    acc_ref,
    s_ref,
    p_ref,
    comp_ref,
    mix,
    sq,
    load_sem,
    recv_sem,
    up_sem,
    across_sem,
    tp_send,
    tp_recv,
):
    rows, width, hs, kvl, group, total_cols, tps = dims
    chips = n // 2
    nq = rows // SEL_BLOCK
    qcols = kvl * group * hs
    cmp_rows = rows // CMP_LEN
    lanes_q = group * rows
    me = lax.axis_index("kv")
    tp = lax.axis_index("tp")
    z = me // 2
    core = me - 2 * z
    mate = 2 * z + 1 - core
    has_up = z < chips - 1
    parts = 3

    kcols = kvl * hs
    joint = kcols % 128 == 0
    if joint:
        kw = weights.at[:, pl.ds(qcols, kcols)]
        vw = weights.at[:, pl.ds(qcols + kcols, kcols)]
    chunks = load_sem.shape[0] // 3 - 2
    step_w = width // chunks
    spots = [pl.ds(c * step_w, step_w) for c in range(chunks)]
    first_loads = []
    for c, spot in enumerate(spots):
        first_loads.append(
            [
                pltpu.make_async_copy(
                    tok_hbm.at[:, spot], tok.at[:, spot], load_sem.at[6 + 3 * c]
                ),
                pltpu.make_async_copy(kw_hbm.at[spot], kw.at[spot], load_sem.at[7 + 3 * c]),
                pltpu.make_async_copy(vw_hbm.at[spot], vw.at[spot], load_sem.at[8 + 3 * c]),
            ]
        )
    for group_loads in first_loads:
        for load in group_loads:
            load.start()
    load_sqk = pltpu.make_async_copy(sqk_hbm, sqk, load_sem.at[0])
    load_sqv = pltpu.make_async_copy(sqv_hbm, sqv, load_sem.at[1])
    load_qw = pltpu.make_async_copy(qw_hbm, weights.at[:, pl.ds(0, qcols)], load_sem.at[2])
    load_gw = pltpu.make_async_copy(gw_hbm, gw, load_sem.at[3])
    load_ow = pltpu.make_async_copy(ow_hbm, ow, load_sem.at[4])
    load_gain = pltpu.make_async_copy(gain_hbm, gain_ref, load_sem.at[5])

    barrier = pltpu.get_barrier_semaphore()
    pl.semaphore_signal(barrier, inc=1, device_id={"kv": mate}, device_id_type=MESH)
    for d in range(1, tps):
        pl.semaphore_signal(
            barrier, inc=1, device_id={"tp": lax.rem(tp + d, tps)}, device_id_type=MESH
        )

    @pl.when(z > 0)
    def _():
        pl.semaphore_signal(barrier, inc=1, device_id={"kv": me - 2}, device_id_type=MESH)

    ids = chosen_ref[...]

    def make_bias(j, carry):
        for b in range(nq):
            hit = jnp.max(jnp.where(ids == j * nq + b, 0.0, NEGATIVE), axis=1, keepdims=True)
            hit = jnp.broadcast_to(hit, (nq, SEL_BLOCK))
            bias[j, b : b + 1, :] = jnp.concatenate(
                [hit[i : i + 1, :] for i in range(nq)] * group, axis=1
            )
        return carry

    lax.fori_loop(0, me + 1, make_bias, 0)

    def clear(j, carry):
        summ[j] = jnp.zeros((cmp_rows, 2 * kcols), jnp.float32)
        return carry

    lax.fori_loop(me + 1, n, clear, 0)

    totals = [None, None]
    for c, spot in enumerate(spots):
        for load in first_loads[c]:
            load.wait()
        if c == 0:
            for load in (load_sqk, load_sqv, load_qw, load_gw, load_ow, load_gain):
                load.start()
        piece_tok = tok[:, spot]
        if joint:
            got = jnp.dot(
                piece_tok,
                weights[spot, qcols : qcols + 2 * kcols],
                preferred_element_type=jnp.float32,
            )
            got = [got[:, :kcols], got[:, kcols:]]
        else:
            got = [
                jnp.dot(piece_tok, w[spot, :], preferred_element_type=jnp.float32)
                for w in (kw, vw)
            ]
        totals = [g if t is None else t + g for t, g in zip(totals, got)]
    sides = totals
    sides = [side.astype(jnp.bfloat16).astype(jnp.float32) for side in sides]
    for i, side in enumerate(sides):
        if not joint:
            side = jnp.concatenate([side, jnp.zeros((rows, 128 - kcols), jnp.float32)], axis=1)
        kvf[i] = side
    keys[me] = sides[0].astype(jnp.bfloat16)
    vals[me] = sides[1].T.astype(jnp.bfloat16)

    def piece(source, part):
        return (keys, summ, vals)[part].at[source]

    def upward(source, part):
        return pltpu.make_async_remote_copy(
            src_ref=piece(source, part),
            dst_ref=piece(source, part),
            send_sem=up_sem.at[source // 2, part],
            recv_sem=recv_sem.at[source, part],
            device_id={"kv": me + 2},
            device_id_type=MESH,
        )

    def across(source, part):
        return pltpu.make_async_remote_copy(
            src_ref=piece(source, part),
            dst_ref=piece(source, part),
            send_sem=across_sem.at[source // 2, part],
            recv_sem=recv_sem.at[source, part],
            device_id={"kv": mate},
            device_id_type=MESH,
        )

    pl.semaphore_wait(barrier, tps + jnp.minimum(chips - 1 - z, 1))

    def send_own(part):
        @pl.when(has_up)
        def _():
            upward(me, part).start()

        @pl.when(core == 0)
        def _():
            across(me, part).start()

    send_own(0)

    load_sqk.wait()
    load_sqv.wait()
    squeezed = []
    for side, weight in ((0, sqk), (1, sqv)):
        tiles = []
        for p in range(0, CMP_LEN, 2):
            a = kvf[side, pl.ds(p, cmp_rows, stride=CMP_LEN), :]
            b = kvf[side, pl.ds(p + 1, cmp_rows, stride=CMP_LEN), :]
            heads = [
                jnp.concatenate([x[:, k * hs : (k + 1) * hs] for x in (a, b)], axis=1)
                for k in range(kvl)
            ]
            tiles.append(jnp.concatenate(heads, axis=0))
        flat = jnp.concatenate(tiles, axis=1).astype(jnp.bfloat16)
        squeezed.append(
            lax.dot_general(flat, weight[...], NT, preferred_element_type=jnp.float32)
            .astype(jnp.bfloat16)
            .astype(jnp.float32)
        )
    summ[me] = jnp.concatenate(
        [
            half[k * cmp_rows : (k + 1) * cmp_rows]
            for half in squeezed
            for k in range(kvl)
        ],
        axis=1,
    )
    send_own(1)
    send_own(2)

    load_qw.wait()
    scale = hs ** (-0.5)
    queries = (
        jnp.dot(tok[...], weights[:, :qcols], preferred_element_type=jnp.float32)
        .astype(jnp.bfloat16)
        .astype(jnp.float32)
        * scale
    )
    turned = queries.T.astype(jnp.bfloat16)
    for k in range(kvl):
        q[k] = jnp.zeros((kcols, lanes_q), jnp.bfloat16)
        for g in range(group):
            h = k * group + g
            q[k, k * hs : (k + 1) * hs, g * rows : (g + 1) * rows] = turned[
                h * hs : (h + 1) * hs, :
            ]
    load_gw.wait()
    hl = kvl * group
    every = jax.nn.sigmoid(
        lax.dot_general(gw[...], tok[...], NT, preferred_element_type=jnp.float32)
    )
    for branch in range(2):
        base = branch * tps * hl
        mine = every[base : base + hl, :]
        for t in range(1, tps):
            mine = jnp.where(tp == t, every[base + t * hl : base + (t + 1) * hl, :], mine)
        gates[branch, 0:hl, :] = mine

    def weigh(source, first, slot=0):
        for k in range(kvl):
            s_ref[k] = jnp.dot(keys[source], q[k], preferred_element_type=jnp.float32)
        alphas = []
        for k in range(kvl):
            for tile in range(lanes_q // 128):
                at = pl.ds(tile * 128, 128)
                xs = []
                for b in range(nq):
                    x = s_ref[k, b * SEL_BLOCK : (b + 1) * SEL_BLOCK, at]
                    x = x + bias[source, b : b + 1, at]
                    if first:
                        col = lax.broadcasted_iota(jnp.int32, (SEL_BLOCK, 128), 1)
                        row = lax.broadcasted_iota(jnp.int32, (SEL_BLOCK, 128), 0)
                        seen = row + b * SEL_BLOCK <= col + (tile * 128) % rows
                        x = jnp.where(seen, x, NEGATIVE)
                    xs.append(x.reshape(SEL_BLOCK // 8, 8, 128))
                top = functools.reduce(jnp.maximum, [jnp.max(x, axis=0) for x in xs])
                peak = jnp.max(top, axis=0, keepdims=True)
                if not first:
                    before = m_ref[k, 0:1, at]
                    peak = jnp.maximum(before, peak)
                    alphas.append(jnp.exp(before - peak))
                total = None
                for b in range(nq):
                    p = jnp.exp(xs[b] - peak)
                    part = jnp.sum(p, axis=0)
                    total = part if total is None else total + part
                    p_ref[slot, k, b * SEL_BLOCK : (b + 1) * SEL_BLOCK, at] = p.reshape(
                        SEL_BLOCK, 128
                    ).astype(jnp.bfloat16)
                if not first:
                    total = total + l_ref[k, :, at] * alphas[-1]
                m_ref[k, 0:1, at] = peak
                l_ref[k, :, at] = total
        return alphas

    def gather(source, alphas, slot=0):
        for k in range(kvl):
            got = jnp.dot(
                vals[source, k * hs : (k + 1) * hs, :],
                p_ref[slot, k],
                preferred_element_type=jnp.float32,
            )
            if alphas:
                tiles = lanes_q // 128
                alpha = jnp.concatenate(alphas[k * tiles : (k + 1) * tiles], axis=1)
                got = got + acc_ref[k] * alpha
            acc_ref[k] = got

    gather(me, weigh(me, True))

    cols = n * cmp_rows

    def compress():
        small = summ[...].reshape(cols, 2 * kcols)
        small_keys = small[:, :kcols].astype(jnp.bfloat16)
        small_vals = small.T[kcols:, :].astype(jnp.bfloat16)
        col = lax.broadcasted_iota(jnp.int32, (cols, rows), 0)
        row = lax.broadcasted_iota(jnp.int32, (cols, rows), 1)
        seen = col * CMP_LEN + (CMP_LEN - 1) <= row + me * rows
        for k in range(kvl):
            s = jnp.dot(small_keys, q[k], preferred_element_type=jnp.float32)
            for g in range(group):
                x = jnp.where(seen, s[:, g * rows : (g + 1) * rows], NEGATIVE)
                peak = jnp.max(x, axis=0, keepdims=True)
                w = jnp.where(seen, jnp.exp(x - peak), 0.0)
                total = jnp.maximum(jnp.sum(w, axis=0, keepdims=True), 1.0)
                comp = jnp.dot(
                    small_vals[k * hs : (k + 1) * hs, :],
                    w.astype(jnp.bfloat16),
                    preferred_element_type=jnp.float32,
                )
                h = k * group + g
                comp_ref[k, :, g * rows : (g + 1) * rows] = comp * (
                    gates[0, h : h + 1, :] / total
                )

    @pl.when(core == 1)
    def _():
        across(me - 1, 0).wait_recv()
        alphas = weigh(me - 1, False)
        across(me - 1, 1).wait_recv()
        across(me - 1, 2).wait_recv()
        gather(me - 1, alphas)

    @pl.when(z == 0)
    def _():
        compress()

    def step(s, carry):
        mine = me - 2 * s
        other = mate - 2 * s

        def take(part):
            upward(mine, part).wait_recv()

            @pl.when(has_up)
            def _():
                upward(mine, part).start()

            across(mine, part).start()

        take(0)
        alphas = weigh(mine, False)
        take(1)
        across(other, 0).wait_recv()
        alphas_other = weigh(other, False, 1)
        across(other, 1).wait_recv()

        @pl.when(s == z)
        def _():
            compress()

        take(2)
        gather(mine, alphas)
        across(other, 2).wait_recv()
        gather(other, alphas_other, 1)
        return carry

    lax.fori_loop(1, z + 1, step, 0)

    def swap(ref, d, source, kind):
        return pltpu.make_async_remote_copy(
            src_ref=ref.at[source],
            dst_ref=ref.at[source],
            send_sem=tp_send.at[kind, d],
            recv_sem=tp_recv.at[kind, source // (kvl if kind < kvl else 1)],
            device_id={"tp": lax.rem(tp + d, tps)},
            device_id_type=MESH,
        )

    for k in range(kvl):
        sel = acc_ref[k] / jnp.sum(l_ref[k], axis=0, keepdims=True)
        mixed = []
        for g in range(group):
            h = k * group + g
            at = slice(g * rows, (g + 1) * rows)
            mixed.append(comp_ref[k, :, at] + gates[1, h : h + 1, :] * sel[:, at])
        mix[tp * kvl + k] = jnp.concatenate(mixed, axis=0).T.astype(jnp.bfloat16)
        for d in range(1, tps):
            swap(mix, d, tp * kvl + k, k).start()
    load_ow.wait()
    load_gain.wait()
    tall = group * hs

    def product(t, k):
        at = pl.ds(pl.multiple_of((t * kvl + k) * tall, tall), tall)
        return jnp.dot(mix[t * kvl + k], ow[at, :], preferred_element_type=jnp.float32)

    proj = product(tp, 0)
    for k in range(1, kvl):
        proj = proj + product(tp, k)
    for k in range(kvl):
        for d in range(1, tps):
            t = lax.rem(tp + d, tps)
            swap(mix, d, t * kvl + k, k).wait_recv()
            proj = proj + product(t, k)
    lanes = proj[:, :128] * proj[:, :128]
    for i in range(1, proj.shape[1] // 128):
        tile = proj[:, i * 128 : (i + 1) * 128]
        lanes = lanes + tile * tile
    sq[tp] = jnp.sum(lanes.T.reshape(16, 8, rows), axis=0)
    for d in range(1, tps):
        swap(sq, d, tp, kvl).start()

    for part in range(parts):
        @pl.when(has_up)
        def _():
            upward(me, part).wait_send()

        @pl.when(core == 0)
        def _():
            across(me, part).wait_send()

    def drain(s, carry):
        mine = me - 2 * s
        for part in range(parts):
            @pl.when(has_up)
            def _():
                upward(mine, part).wait_send()

            across(mine, part).wait_send()
        return carry

    lax.fori_loop(1, z + 1, drain, 0)
    for d in range(1, tps):
        swap(sq, d, lax.rem(tp + d, tps), kvl).wait_recv()
    squares = jnp.sum(jnp.sum(sq[...], axis=0), axis=0, keepdims=True)
    factor = lax.rsqrt(squares / total_cols + EPSILON)
    column = jnp.broadcast_to(factor, (128, rows)).T
    width_out = out_ref.shape[1]
    gain_all = gain_ref[...].astype(jnp.float32).reshape(1, total_cols)
    gain = gain_all[:, :width_out]
    for t in range(1, tps):
        gain = jnp.where(tp == t, gain_all[:, t * width_out : (t + 1) * width_out], gain)
    for i in range(width_out // 128):
        at = slice(i * 128, (i + 1) * 128)
        out_ref[:, at] = (proj[:, at] * column * gain[:, at]).astype(out_ref.dtype)
    for d in range(1, tps):
        for k in range(kvl):
            swap(mix, d, tp * kvl + k, k).wait_send()
        swap(sq, d, tp, kvl).wait_send()


def body(
    n,
    tps,
    tokens,
    query_weight,
    key_weight,
    value_weight,
    gate_weight,
    squeeze_key,
    squeeze_value,
    out_weight,
    out_gain,
    chosen,
):
    rows, width = tokens.shape
    hs = squeeze_key.shape[1]
    kvl = key_weight.shape[1] // hs
    qcols = query_weight.shape[1]
    group = qcols // hs // kvl
    cols = out_weight.shape[1]
    total_cols = out_gain.shape[0]
    lanes_q = group * rows
    cmp_rows = rows // CMP_LEN
    dims = (rows, width, hs, kvl, group, total_cols, tps)
    kcols = kvl * hs
    joint = kcols % 128 == 0
    spare = (8, 128) if joint else (width, kcols)
    any_spec = pl.BlockSpec(memory_space=pl.ANY)
    vmem = pl.BlockSpec(memory_space=pltpu.VMEM)
    bf, f32 = jnp.bfloat16, jnp.float32
    dma = pltpu.SemaphoreType.DMA
    return pl.pallas_call(
        functools.partial(kernel, n, dims),
        out_shape=jax.ShapeDtypeStruct((rows, cols), bf),
        in_specs=[vmem] + [any_spec] * 9,
        out_specs=vmem,
        scratch_shapes=[
            pltpu.VMEM((rows, width), bf),
            pltpu.VMEM((width, qcols + 2 * kcols if joint else qcols), bf),
            pltpu.VMEM(spare, bf),
            pltpu.VMEM(spare, bf),
            pltpu.VMEM((gate_weight.shape[0] * gate_weight.shape[2], width), bf),
            pltpu.VMEM(squeeze_key.shape[::-1], bf),
            pltpu.VMEM(squeeze_value.shape[::-1], bf),
            pltpu.VMEM(out_weight.shape, bf),
            pltpu.VMEM(out_gain.shape, bf),
            pltpu.VMEM((n, rows, kcols), bf),
            pltpu.VMEM((n, kcols, rows), bf),
            pltpu.VMEM((2, rows, max(kcols, 128)), f32),
            pltpu.VMEM((n, cmp_rows, 2 * kcols), f32),
            pltpu.VMEM((n, 8, lanes_q), f32),
            pltpu.VMEM((kvl, kcols, lanes_q), bf),
            pltpu.VMEM((2, 8, rows), f32),
            pltpu.VMEM((kvl, 8, lanes_q), f32),
            pltpu.VMEM((kvl, 8, lanes_q), f32),
            pltpu.VMEM((kvl, hs, lanes_q), f32),
            pltpu.VMEM((kvl, rows, lanes_q), f32),
            pltpu.VMEM((2, kvl, rows, lanes_q), bf),
            pltpu.VMEM((kvl, hs, lanes_q), f32),
            pltpu.VMEM((tps * kvl, rows, group * hs), bf),
            pltpu.VMEM((tps, 8, rows), f32),
            dma((18,)),
            dma((n, 3)),
            dma((n // 2, 3)),
            dma((n // 2, 3)),
            dma((kvl + 1, tps)),
            dma((kvl + 1, tps)),
        ],
        compiler_params=pltpu.CompilerParams(
            collective_id=0, has_side_effects=True, vmem_limit_bytes=56 * 1024 * 1024
        ),
    )(
        chosen,
        tokens,
        query_weight,
        key_weight,
        value_weight,
        gate_weight.transpose(0, 2, 1).reshape(-1, width),
        squeeze_key.T,
        squeeze_value.T,
        out_weight,
        out_gain,
    )


def solution(mesh):
    in_specs = (
        P(("grp", "kv"), None),
        P(None, "tp"),
        P(None, "tp"),
        P(None, "tp"),
        P(),
        P(),
        P(),
        P(None, "tp"),
        P(),
        P(("grp", "kv"), None),
    )
    return jax.shard_map(
        functools.partial(body, mesh.shape["kv"], mesh.shape["tp"]),
        mesh=mesh,
        in_specs=in_specs,
        out_specs=P(("grp", "kv"), "tp"),
        check_vma=False,
    )
```
